32 devices in a mesh: sp: 16 (over z, y, x), tp: 2 (over core).
Axes of the slice: x: 2, y: 2, z: 4, core: 2. Of those that a mesh axis runs over, the one named last changes fastest.
Arguments:
- residual: bfloat16 [4096, 2048], P(('sp', 'tp')), may hold values from -6 to 6
- query_rows: bfloat16 [4096, 1024], P('sp', 'tp'), may hold values from -141 to 141
- key_rows: bfloat16 [4096, 1024], P('sp', 'tp'), may hold values from -7.8 to 7.8
- value_rows: bfloat16 [4096, 1024], P('sp', 'tp'), may hold values from -6 to 6
- mix_lambda: float32 [8], P('tp'), may hold values from 0.3 to 0.8
- documents: int32 [4096], P('sp'), may hold values from 0 to 7, never falling along the last dimension, each value on 1 to 768 neighbouring positions
- out_weight: bfloat16 [1024, 2048], replicated, may hold values from -0.1875 to 0.1875
- norm_gain: float32 [2048], replicated, may hold values from 0.1 to 1.9
- gate_weight: bfloat16 [16, 2048, 2048], P('sp', None, 'tp'), may hold values from -0.125 to 0.125
- up_weight: bfloat16 [16, 2048, 2048], P('sp', None, 'tp'), may hold values from -0.125 to 0.125
- down_weight: bfloat16 [16, 2048, 2048], P('sp', 'tp'), may hold values from -0.125 to 0.125
- routes: int32 [4096, 2], P(('sp', 'tp')), may hold values from 0 to 15, all different within a row; in each aligned block of 128 rows (0 to 127, 128 to 255, ...) at most 32 rows name the same one
- route_weights: float32 [4096, 2], P(('sp', 'tp')), may hold values from 0.25 to 1
Outputs:
- layer_out: bfloat16 [4096, 2048], P(('sp', 'tp'))
The draws below stay inside these ranges and needn't reach their ends.
Inputs may be any that keep to these rules, and one draw needn't show every extreme that they name: `documents`: document numbers never fall along the sequence; a document covers at most 768 positions, and one covers exactly that many. `routes`: each row names two different experts. Among the rows of one index of sp+tp, no expert is named by more than 32 rows, and in every draw some expert is named by exactly 32 rows of some such block.
All inputs are finite; a program needn't handle non-finite values.
Results may differ from the reference program's by a relative error of at most 0.013.
Values may be sent and summed in bfloat16 or wider, within the bound.
No kernel may reach another device: no remote copies, remote signals or barrier semaphores. Data moves between devices by JAX's collectives and lax.ppermute only.
A program may use at most 128 MiB of HBM per device.

```python
import math
import jax
import jax.numpy as jnp
import numpy as np
from jax import lax

D = 2048
HEADS = 8
HD = 64
VD = 128
FFE = 2048
TOK_DEV = 256
REACH = 3
TOKENS = 4096
EXPERTS = 16
CAP = 32
DOCS = 8
N_SP = 16
N_TP = 2


def drawn_pair(key):
    shape_rows = (TOKENS, HEADS * 2 * HD)
    base_query = jnp.clip(1.3 * jax.random.normal(jax.random.fold_in(key, 101), shape_rows, jnp.float32), -7.8, 7.8)
    base_keys = jnp.clip(1.3 * jax.random.normal(jax.random.fold_in(key, 102), shape_rows, jnp.float32), -7.8, 7.8)
    return (base_query, base_keys)


def draw_query_rows(key, part):
    return drawn_pair(key)[0].astype(jnp.bfloat16)


def draw_key_rows(key, part):
    return drawn_pair(key)[1].astype(jnp.bfloat16)


def steps_of(rng, dims, pieces, low, high):
    factor_of, own = 1.0, jax.random.fold_in(rng, 6)
    for axis_at, parts in pieces:
        steps = jnp.exp(jax.random.uniform(jax.random.fold_in(own, axis_at), (parts,), jnp.float32, low / len(pieces), high / len(pieces)))
        factor_of = factor_of * jnp.repeat(steps, dims[axis_at] // parts).reshape([-1 if axis == axis_at else 1 for axis in range(len(dims))])
    return factor_of


def split_up(count, total, most, slope):
    loads = [(1 << 20) // math.isqrt(rank ** slope) + 1 for rank in range(2, count + 1)]
    rest, counts = total - most - (count - 1), [1] * (count - 1)
    while rest > 0:
        candidates = [i for i in range(count - 1) if counts[i] < most]
        pool, remaining = sum([loads[i] for i in candidates]), rest
        for i in candidates:
            addition = min(most - counts[i], max(1, remaining * loads[i] // pool), rest)
            counts[i] = counts[i] + addition
            rest = rest - addition
    return np.array([most] + counts)


def uneven_parts(rng, amount, total, limit, lean):
    if amount == 2:
        one = jax.random.randint(rng, (), max(1, total - limit), min(limit, total - 1) + 1)
        return jnp.stack([one, total - one])
    lengths = jnp.asarray(split_up(amount, total, limit, lean), jnp.int32)
    pairs = (amount - 1) // 2
    donor, receiver = lengths[1:1 + 2 * pairs:2], lengths[2:2 + 2 * pairs:2]
    slack = jnp.minimum(donor - 1, limit - receiver)
    shifted = jax.random.randint(jax.random.fold_in(rng, 1), (pairs,), 0, 1 << 20) % (slack + 1)
    lengths = lengths.at[1:1 + 2 * pairs:2].set(donor - shifted).at[2:2 + 2 * pairs:2].set(receiver + shifted)
    return lengths[jax.random.permutation(jax.random.fold_in(rng, 2), amount)]


def assign_block(own_key, own, number, rows, count, top, reach, lean):
    ranking = jax.random.permutation(own_key, count)
    crowded, usual = portions_of(count, rows * top, reach, lean, True), portions_of(count, rows * top, reach, lean, False)
    places = jnp.arange(count)

    def named(sizes, offset_by):
        used = int((sizes > 0).sum())
        fixed = max(1, used // 4)
        passed = fixed + (places - fixed + offset_by * (used - fixed)) % max(1, count - fixed)
        return jnp.zeros((count,), jnp.int32).at[ranking[jnp.where(places < fixed, places, passed)]].set(jnp.asarray(sizes, jnp.int32))

    sizes = jnp.where(number % 4 == 0, named(crowded, number // 4), named(usual, number - number // 4 - 1))
    mixed = jax.random.permutation(jax.random.fold_in(own, 3), count)
    donor, sink = mixed[0:count // 2 * 2:2], mixed[1:count // 2 * 2:2]
    slack = jnp.minimum(sizes[donor] - 1, reach - sizes[sink]) // 2
    slack = jnp.where((donor == ranking[0]) | (sink == ranking[0]) | (sizes[sink] == 0), 0, jnp.maximum(slack, 0))
    passed = jax.random.randint(jax.random.fold_in(own, 4), (count // 2,), 0, 1 << 20) % (slack + 1)
    sizes = sizes.at[donor].add(-passed).at[sink].add(passed)
    items = jnp.searchsorted(jnp.cumsum(sizes), jnp.arange(rows * top), side="right").astype(jnp.int32)
    table = items.reshape(top, rows).T
    table = table[jax.random.permutation(jax.random.fold_in(own, 1), rows)]
    offset_by = jax.random.randint(jax.random.fold_in(own, 2), (rows, 1), 0, top)
    return jnp.take_along_axis(table, (jnp.arange(top)[None, :] + offset_by) % top, axis=1)


def portions_of(amount, total, reach, slope, full):
    weights = [(1 << 20) // math.isqrt(grade ** slope) + 1 for grade in range(1, amount + 1)]
    largest = reach if full else min(reach, max(-(-total // amount), total * weights[0] // sum(weights)))
    least = 1 if total - largest >= amount - 1 else 0
    holding, rest = [largest] + [least] * (amount - 1), total - largest - least * (amount - 1)
    while rest > 0:
        candidates = [i for i in range(1, amount) if holding[i] < largest] or [i for i in range(1, amount) if holding[i] < reach]
        pool, budget = sum([weights[i] for i in candidates]), rest
        for i in candidates:
            more = min(reach - holding[i], max(1, budget * weights[i] // pool), rest)
            holding[i] = holding[i] + more
            rest = rest - more
    return np.array(holding)


def normal_values(own_key, shape, deviation, limit, cuts=(), held_as=jnp.bfloat16):
    level = steps_of(own_key, shape, cuts, -0.22, 0.18) if cuts else 1.0
    values = jax.random.normal(own_key, shape, jnp.float32) * deviation * level
    return jnp.minimum(jnp.maximum(values, -limit), limit).astype(held_as)


def setup_inputs(seed: int = 0) -> dict:
    keys = jax.random.split(jax.random.key(seed), 14)
    residual = normal_values(keys[0], (TOKENS, D), 1.0, 6.0, ((0, 32),))
    query_rows = draw_query_rows(jax.random.fold_in(keys[13], 71), 0)
    key_rows = draw_key_rows(jax.random.fold_in(keys[13], 71), 0)
    value_rows = normal_values(keys[3], (TOKENS, HEADS * VD), 1.0, 6.0, ((0, 16), (1, 2)))
    mix_lambda = jnp.clip(0.3 + 0.5 * jax.random.uniform(keys[4], (HEADS,), jnp.float32) ** steps_of(keys[4], (HEADS,), ((0, 2),), -0.2, 0.2), 0.3, 0.8)
    documents = jnp.searchsorted(jnp.cumsum(uneven_parts(keys[5], DOCS, TOKENS, REACH * TOK_DEV, 0)), jnp.arange(TOKENS), side="right").astype(jnp.int32)
    out_weight = normal_values(keys[6], (HEADS * VD, D), (HEADS * VD) ** -0.5, 0.1875)
    norm_gain = jnp.clip(1.0 + 0.18 * jax.random.normal(keys[7], (D,), jnp.float32), 0.1, 1.9)
    gate_weight = normal_values(keys[8], (EXPERTS, D, FFE), D ** -0.5, 0.125, ((0, 16), (2, 2)))
    up_weight = normal_values(keys[9], (EXPERTS, D, FFE), D ** -0.5, 0.125, ((0, 16), (2, 2)))
    down_weight = normal_values(keys[10], (EXPERTS, FFE, D), FFE ** -0.5, 0.125, ((0, 16), (1, 2)))
    routes_keys = jax.random.split(jax.random.fold_in(keys[11], 1), TOKENS // (TOK_DEV // 2))
    routes_turns = jax.random.permutation(jax.random.fold_in(keys[11], 3), TOKENS // (TOK_DEV // 2))
    routes = jax.vmap(lambda own, number: assign_block(jax.random.fold_in(keys[11], 2), own, number, TOK_DEV // 2, EXPERTS, 2, CAP, 2))(routes_keys, routes_turns).reshape((TOKENS, 2))
    route_weights = jnp.clip(0.25 + 0.75 * jax.random.uniform(keys[12], (TOKENS, 2), jnp.float32) ** steps_of(keys[12], (TOKENS, 2), ((0, 32),), -0.2, 0.2), 0.25, 1.0)
    return {"residual": residual, "query_rows": query_rows, "key_rows": key_rows, "value_rows": value_rows, "mix_lambda": mix_lambda, "documents": documents, "out_weight": out_weight, "norm_gain": norm_gain, "gate_weight": gate_weight, "up_weight": up_weight, "down_weight": down_weight, "routes": routes, "route_weights": route_weights}


def rms_rows(values_in):
    return values_in * lax.rsqrt(lax.optimization_barrier(jnp.mean(values_in * values_in, axis=-1, keepdims=True)) + 1e-06)

def reference(residual, query_rows, key_rows, value_rows, mix_lambda, documents, out_weight, norm_gain, gate_weight, up_weight, down_weight, routes, route_weights):
    score_scale = HD ** (-0.5)
    queries = query_rows.reshape(TOKENS // TOK_DEV, TOK_DEV, HEADS, 2, HD)
    all_keys = key_rows.reshape(TOKENS, HEADS, 2, HD).astype(jnp.float32)
    all_values = value_rows.reshape(TOKENS, HEADS, VD).astype(jnp.float32)
    block_ids = documents.reshape(TOKENS // TOK_DEV, TOK_DEV)

    def attend(operands):
        block_query, query_ids = operands
        scores = jnp.einsum('qhcd,khcd->hcqk', block_query.astype(jnp.float32), all_keys) * score_scale
        same_document = query_ids[:, None] == documents[None, :]
        masked = jnp.where(same_document[None, None], scores, -1e+30)
        largest = lax.optimization_barrier(jnp.max(masked, axis=-1, keepdims=True))
        lifted = jnp.exp(masked - largest)
        probabilities = lifted / lax.optimization_barrier(jnp.sum(lifted, axis=-1, keepdims=True))
        weights = (probabilities[:, 0] - mix_lambda[:, None, None] * probabilities[:, 1]).astype(jnp.bfloat16)
        head_out = jnp.einsum('hqk,khd->qhd', weights.astype(jnp.float32), all_values)
        head_normed = rms_rows(head_out).astype(jnp.bfloat16)
        return head_normed.reshape(TOK_DEV, HEADS * VD)
    head_rows = lax.map(attend, (queries, block_ids)).reshape(TOKENS, HEADS * VD)
    projected = jnp.dot(head_rows, out_weight, preferred_element_type=jnp.float32)
    mixed = (residual.astype(jnp.float32) + projected).astype(jnp.bfloat16)
    normed = (rms_rows(mixed.astype(jnp.float32)) * norm_gain).astype(jnp.bfloat16)
    top_count = routes.shape[1]
    assign_count = TOKENS * top_count
    flat_routes = routes.reshape(-1)
    padded_rows = jnp.concatenate([normed, jnp.zeros((1, D), jnp.bfloat16)], axis=0)
    most_rows = N_SP * N_TP * CAP
    half_width = FFE // N_TP

    def one_expert(collected, expert):
        chosen = jnp.nonzero(flat_routes == expert, size=most_rows, fill_value=assign_count)[0].astype(jnp.int32)
        picked = padded_rows[chosen // top_count]
        gate = jnp.dot(picked, gate_weight[expert], preferred_element_type=jnp.float32)
        upward = jnp.dot(picked, up_weight[expert], preferred_element_type=jnp.float32)
        hidden = (jax.nn.silu(gate) * upward).astype(jnp.bfloat16)
        hidden_halves = hidden.reshape(most_rows, N_TP, half_width).astype(jnp.float32)
        down_halves = down_weight[expert].reshape(N_TP, half_width, D).astype(jnp.float32)
        partial_value = jnp.einsum('rhp,hpd->hrd', hidden_halves, down_halves).astype(jnp.bfloat16)
        expert_out = lax.optimization_barrier(jnp.sum(partial_value.astype(jnp.float32), axis=0)).astype(jnp.bfloat16)
        return (collected.at[chosen].set(expert_out), None)
    collected, _ = lax.scan(one_expert, jnp.zeros((assign_count + 1, D), jnp.bfloat16), jnp.arange(EXPERTS, dtype=jnp.int32))
    outputs = collected[:assign_count].reshape(TOKENS, top_count, D).astype(jnp.float32)
    weighted = lax.optimization_barrier(jnp.sum(outputs * route_weights[:, :, None], axis=1))
    return (mixed.astype(jnp.float32) + weighted).astype(jnp.bfloat16)
```

```python
import functools

import jax
import jax.numpy as jnp
from jax import lax
from jax.experimental import pallas as pl
from jax.experimental.pallas import tpu as pltpu
from jax.sharding import PartitionSpec as P

HD = 64
REACH = 3
EPS = 1e-06
BF = jnp.bfloat16
F32 = jnp.float32
VM = pl.BlockSpec(memory_space=pltpu.VMEM)
SM = pl.BlockSpec(memory_space=pltpu.SMEM)
ANY = pl.BlockSpec(memory_space=pl.ANY)
PARAMS = pltpu.CompilerParams(vmem_limit_bytes=56 * 1024 * 1024)


def cost(flops, bytes_accessed):
    return pl.CostEstimate(flops=flops, bytes_accessed=bytes_accessed, transcendentals=0)


def pack_kernel(q_ref, k_ref, v_ref, id_ref, qo_ref, kv_ref):
    heads, length, width = qo_ref.shape
    for h in range(heads):
        columns = slice(h * width, (h + 1) * width)
        qo_ref[h] = (q_ref[:, columns].astype(F32) * (HD**-0.5)).astype(BF)
        kv_ref[h, :length, :width] = k_ref[:, columns]
        kv_ref[h, :length, width:] = v_ref[:, columns]
        kv_ref[h, length:, :] = jnp.broadcast_to(id_ref[...], kv_ref[h, length:, :].shape)


def pack(query_rows, key_rows, value_rows, id_row, heads):
    length = query_rows.shape[0]
    width = query_rows.shape[1] // heads
    return pl.pallas_call(
        pack_kernel,
        in_specs=[VM] * 4,
        out_specs=[VM, VM],
        out_shape=[
            jax.ShapeDtypeStruct((heads, length, width), BF),
            jax.ShapeDtypeStruct((heads, length + 16, 2 * width), BF),
        ],
        compiler_params=PARAMS,
        name="pack",
    )(query_rows, key_rows, value_rows, id_row)


def attention_kernel(
    lam_ref, q_ref, prev_ref, own_ref, next_ref, o_ref, kv_ref, id_ref, s_ref, m_ref, l_ref, a_ref
):
    b = pl.program_id(0)
    length, width = o_ref.shape[1:]
    before, group, after = prev_ref.shape[0], own_ref.shape[0], next_ref.shape[0]
    span = before + 1 + after

    @pl.when(b == 0)
    def _():
        id_ref[...] = jnp.zeros_like(id_ref)
        for first, ref in ((0, prev_ref), (before, own_ref), (before + group, next_ref)):
            for i in range(ref.shape[0]):
                kv_ref[first + i] = ref[i, :length, :]
                id_ref[first + i : first + i + 1, :] = ref[i, length : length + 16, :].astype(F32)[:1]

    query_ids = id_ref[pl.ds(b + before, 1), :]
    low = jnp.min(query_ids, axis=1, keepdims=True)
    high = jnp.max(query_ids, axis=1, keepdims=True)
    ids = id_ref[...]
    smallest = jnp.min(ids, axis=1, keepdims=True)
    largest = jnp.max(ids, axis=1, keepdims=True)
    place = lax.broadcasted_iota(jnp.int32, smallest.shape, 0) - b
    apart = (largest < low) | (smallest > high)
    left = jnp.sum(jnp.where(apart & (place >= 0) & (place < before), 1.0, 0.0))
    right = jnp.sum(jnp.where(apart & (place > before) & (place < span), 1.0, 0.0))
    start = left.astype(jnp.int32)
    stop = span - right.astype(jnp.int32)
    query_column = jnp.transpose(jnp.broadcast_to(query_ids, (128, length)))

    q = q_ref[b]
    zero = jnp.zeros((length, HD), BF)
    stacked = jnp.concatenate(
        [
            jnp.concatenate([q[:, :HD], zero], axis=1),
            jnp.concatenate([zero, q[:, HD:]], axis=1),
        ],
        axis=0,
    )
    m_ref[...] = jnp.full_like(m_ref, -1e30)
    l_ref[...] = jnp.zeros_like(l_ref)
    a_ref[...] = jnp.zeros_like(a_ref)

    def score(j, carry):
        keys = kv_ref[b + j, :, :width]
        scores = lax.dot_general(
            stacked, keys, (((1,), (1,)), ((), ())), preferred_element_type=F32
        )
        key_ids = id_ref[pl.ds(b + j, 1), :]
        for c in range(2):
            rows = slice(c * length, (c + 1) * length)
            best = m_ref[rows, :]
            for part in range(length // 128):
                columns = slice(part * 128, (part + 1) * 128)
                piece = jnp.where(
                    query_column == key_ids[:, columns], scores[rows, columns], -1e30
                )
                s_ref[j, rows, columns] = piece
                best = jnp.maximum(best, piece)
            m_ref[rows, :] = best
        return carry

    lax.fori_loop(start, stop, score, 0)
    top = jnp.max(m_ref[...], axis=1, keepdims=True)

    def lift(j, carry):
        lifted = jnp.exp(s_ref[j] - top)
        s_ref[j] = lifted
        total = l_ref[...]
        for part in range(length // 128):
            total = total + lifted[:, part * 128 : (part + 1) * 128]
        l_ref[...] = total
        return carry

    lax.fori_loop(start, stop, lift, 0)
    total = jnp.sum(l_ref[...], axis=1, keepdims=True)
    first = 1.0 / total[:length]
    second = lam_ref[0] / total[length:]

    def gather(j, carry):
        weights = (s_ref[j, :length, :] * first - s_ref[j, length:, :] * second).astype(BF)
        a_ref[...] += jnp.dot(weights, kv_ref[b + j, :, width:], preferred_element_type=F32)
        return carry

    lax.fori_loop(start, stop, gather, 0)
    out = a_ref[...]
    scale = lax.rsqrt(jnp.mean(out * out, axis=1, keepdims=True) + EPS)
    o_ref[b] = (out * scale).astype(BF)


def attention(lam, q, prev, own, following):
    group, length, width = q.shape
    before, after = prev.shape[0], following.shape[0]
    span = before + 1 + after
    return pl.pallas_call(
        attention_kernel,
        grid=(group,),
        in_specs=[SM] + [VM] * 4,
        out_specs=VM,
        out_shape=jax.ShapeDtypeStruct((group, length, width), BF),
        scratch_shapes=[
            pltpu.VMEM((before + group + after, length, 2 * width), BF),
            pltpu.VMEM((-(-(before + group + after) // 8) * 8, length), F32),
            pltpu.VMEM((span, 2 * length, length), F32),
            pltpu.VMEM((2 * length, 128), F32),
            pltpu.VMEM((2 * length, 128), F32),
            pltpu.VMEM((length, width), F32),
        ],
        compiler_params=PARAMS,
        cost_estimate=cost(8 * 10**9, 4 * 10**6),
        name="attention",
    )(lam, q, prev, own, following)


def project_kernel(
    heads_ref, residual_ref, gain_ref, meta_ref, weight_ref, mixed_ref, rows_ref, left_ref
):
    n = pl.program_id(0)
    tile = weight_ref.shape[1]
    tokens, width = mixed_ref.shape
    members = heads_ref.shape[0]
    value_dim = heads_ref.shape[2]

    @pl.when(n == 0)
    def _():
        for source in range(members):
            head = (source % 2) * (members // 2) + source // 2
            left_ref[:, head * value_dim : (head + 1) * value_dim] = heads_ref[source]

    columns = pl.ds(pl.multiple_of(n * tile, tile), tile)
    projected = jnp.dot(left_ref[...], weight_ref[...], preferred_element_type=F32)
    mixed_ref[:, columns] = (residual_ref[:, columns].astype(F32) + projected).astype(BF)

    @pl.when(n == pl.num_programs(0) - 1)
    def _():
        wide = mixed_ref[...].astype(F32)
        scale = lax.rsqrt(jnp.mean(wide * wide, axis=1, keepdims=True) + EPS)
        normed = (wide * scale * gain_ref[...]).astype(BF)
        slots = rows_ref.shape[0]
        place = lax.broadcasted_iota(jnp.int32, (slots, tokens), 0).astype(F32)
        pick = (place == meta_ref[0:1, :]) | (place == meta_ref[1:2, :])
        rows_ref[...] = jnp.dot(
            jnp.where(pick, 1.0, 0.0).astype(BF), normed, preferred_element_type=F32
        ).astype(BF)


def project(heads, residual, gain, meta, out_weight, slots, tile=512):
    members, tokens, value_dim = heads.shape
    depth, width = out_weight.shape
    return pl.pallas_call(
        project_kernel,
        grid=(width // tile,),
        in_specs=[VM, VM, VM, VM, pl.BlockSpec((depth, tile), lambda n: (0, n))],
        out_specs=[VM, VM],
        out_shape=[
            jax.ShapeDtypeStruct((tokens, width), BF),
            jax.ShapeDtypeStruct((slots, width), BF),
        ],
        scratch_shapes=[pltpu.VMEM((tokens, depth), BF)],
        compiler_params=PARAMS,
        cost_estimate=cost(3 * 10**9, 8 * 10**6),
        name="project",
    )(heads, residual, gain, meta, out_weight)


def expert_kernel(
    x_ref, g0, u0, d0, g1, u1, d1, y_ref, gb, ub, db, acc_ref, half_ref, sems, *, tile, slots
):
    per_half = g0.shape[1] // tile
    steps = 2 * per_half
    sources = ((g0, u0, d0), (g1, u1, d1))

    def copies(step):
        g, u, d = sources[step // per_half]
        at = (step % per_half) * tile
        slot = step % slots
        return (
            pltpu.make_async_copy(g.at[:, pl.ds(at, tile)], gb.at[slot], sems.at[slot, 0]),
            pltpu.make_async_copy(u.at[:, pl.ds(at, tile)], ub.at[slot], sems.at[slot, 1]),
            pltpu.make_async_copy(d.at[pl.ds(at, tile), :], db.at[slot], sems.at[slot, 2]),
        )

    for step in range(min(slots - 1, steps)):
        for copy in copies(step):
            copy.start()
    for step in range(steps):
        if step + slots - 1 < steps:
            for copy in copies(step + slots - 1):
                copy.start()
        for copy in copies(step):
            copy.wait()
        slot = step % slots
        x = x_ref[...]
        gate = jnp.dot(x, gb[slot], preferred_element_type=F32)
        upward = jnp.dot(x, ub[slot], preferred_element_type=F32)
        hidden = (gate / (1.0 + jnp.exp(-gate)) * upward).astype(BF)
        part = jnp.dot(hidden, db[slot], preferred_element_type=F32)
        if step % per_half == 0:
            acc_ref[...] = part
        else:
            acc_ref[...] += part
        if step == per_half - 1:
            half_ref[...] = acc_ref[...].astype(BF)
    y_ref[...] = (
        half_ref[...].astype(F32) + acc_ref[...].astype(BF).astype(F32)
    ).astype(BF)


def experts_of(x, own, other, tile=256, slots=3):
    rows, width = x.shape
    return pl.pallas_call(
        functools.partial(expert_kernel, tile=tile, slots=slots),
        in_specs=[VM] + [ANY] * 6,
        out_specs=VM,
        out_shape=jax.ShapeDtypeStruct((rows, width), BF),
        scratch_shapes=[
            pltpu.VMEM((slots, width, tile), BF),
            pltpu.VMEM((slots, width, tile), BF),
            pltpu.VMEM((slots, tile, width), BF),
            pltpu.VMEM((rows, width), F32),
            pltpu.VMEM((rows, width), BF),
            pltpu.SemaphoreType.DMA((slots, 3)),
        ],
        compiler_params=PARAMS,
        cost_estimate=cost(9 * 10**9, 26 * 10**6),
        name="experts",
    )(x, *own, *other)


def picked(meta_ref, rows_ref):
    slots = rows_ref.shape[0]
    tokens = meta_ref.shape[1]
    columns = jnp.transpose(meta_ref[...])
    place = lax.broadcasted_iota(jnp.int32, (tokens, slots), 1).astype(F32)
    total = None
    for k in range(2):
        pick = jnp.where(place == columns[:, k : k + 1], 1.0, 0.0).astype(BF)
        rows = jnp.dot(pick, rows_ref[...], preferred_element_type=F32)
        part = rows * columns[:, 2 + k : 3 + k]
        total = part if total is None else total + part
    return total


def partial_kernel(meta_ref, rows_ref, o_ref):
    o_ref[...] = picked(meta_ref, rows_ref).astype(BF)


def final_kernel(meta_ref, rows_ref, mixed_ref, far_ref, o_ref):
    total = picked(meta_ref, rows_ref) + far_ref[...].astype(F32)
    o_ref[...] = (mixed_ref[...].astype(F32) + total).astype(BF)


def partial_sum(meta, rows):
    return pl.pallas_call(
        partial_kernel,
        in_specs=[VM] * 2,
        out_specs=VM,
        out_shape=jax.ShapeDtypeStruct((meta.shape[1], rows.shape[1]), BF),
        compiler_params=PARAMS,
        cost_estimate=cost(10**9, 2 * 10**6),
        name="partial_sum",
    )(meta, rows)


def final_sum(meta, rows, mixed, far):
    return pl.pallas_call(
        final_kernel,
        in_specs=[VM] * 4,
        out_specs=VM,
        out_shape=jax.ShapeDtypeStruct(mixed.shape, BF),
        compiler_params=PARAMS,
        cost_estimate=cost(10**9, 3 * 10**6),
        name="final_sum",
    )(meta, rows, mixed, far)


def ranks_of(routes, experts):
    tokens = routes.shape[0]
    table = (routes[:, :, None] == jnp.arange(experts, dtype=jnp.int32)).astype(F32)
    named = jnp.sum(table, axis=1)
    order = jnp.arange(tokens)
    below = (order[:, None] > order[None, :]).astype(BF)
    earlier = jnp.dot(below, named.astype(BF), preferred_element_type=F32)
    return jnp.sum(earlier[:, None, :] * table, axis=2)


def meta_of(routes, ranks, route_weights, first, count, capacity):
    local = routes - first
    inside = (local >= 0) & (local < count)
    target = jnp.where(inside, local.astype(F32) * capacity + ranks, -1.0)
    rows = jnp.concatenate([target.T, route_weights.T], axis=0)
    return jnp.concatenate([rows, jnp.zeros((8 - rows.shape[0], rows.shape[1]), F32)], axis=0)


def on_device(
    residual,
    query_rows,
    key_rows,
    value_rows,
    mix_lambda,
    documents,
    out_weight,
    norm_gain,
    gate_weight,
    up_weight,
    down_weight,
    routes,
    route_weights,
):
    length = query_rows.shape[0]
    heads = mix_lambda.shape[0]
    width = residual.shape[1]
    count = lax.axis_size("sp")
    twins = lax.axis_size("tp")
    here = lax.axis_index("sp")
    half = count // 2
    capacity = 2 * length // count
    planes = [[g * heads + j for j in range(heads)] for g in range(count // heads)]
    halves = [[h * half + j for j in range(half)] for h in range(2)]
    mirror = [(i, (i + half) % count) for i in range(count)]
    swap = [(i, twins - 1 - i) for i in range(twins)]

    id_row = (documents + 1).astype(BF).reshape(1, length)
    queries, pairs = pack(query_rows, key_rows, value_rows, id_row, heads)
    pairs = lax.all_to_all(pairs, "sp", 0, 0, tiled=True, axis_index_groups=planes)
    prev = lax.ppermute(
        pairs[heads - REACH :], "sp", [(i, i + heads) for i in range(count - heads)]
    )
    following = lax.ppermute(
        pairs[:REACH], "sp", [(i + heads, i) for i in range(count - heads)]
    )
    queries = lax.all_to_all(queries, "sp", 0, 0, tiled=True, axis_index_groups=planes)

    ranks = ranks_of(routes, count)
    my_half = here // half
    meta_own = meta_of(routes, ranks, route_weights, my_half * half, half, capacity)
    meta_far = meta_of(routes, ranks, route_weights, (1 - my_half) * half, half, capacity)
    meta_far = lax.ppermute(meta_far, "sp", mirror)
    residual_late, _ = lax.optimization_barrier((residual, pairs))
    residual_far = lax.ppermute(residual_late, "sp", mirror)

    own = (gate_weight[0], up_weight[0], down_weight[0])
    other = tuple(lax.ppermute(weight, "tp", swap) for weight in own)

    lam = lax.dynamic_slice(mix_lambda, (here % heads,), (1,))
    outs = attention(lam, queries, prev, pairs, following)
    outs = outs.reshape(heads * twins, length // twins, outs.shape[2])
    both = [[g * heads * twins + j for j in range(heads * twins)] for g in range(count // heads)]
    token_heads = lax.all_to_all(
        outs, ("sp", "tp"), 0, 0, tiled=True, axis_index_groups=both
    )
    heads_far = lax.ppermute(token_heads, "sp", mirror)

    gain = norm_gain.reshape(1, width)
    slots = half * capacity

    def exchange(rows):
        rows = rows.reshape(half, capacity, width)
        rows = lax.all_to_all(rows, "sp", 0, 0, tiled=True, axis_index_groups=halves)
        return rows.reshape(slots, width)

    mixed, rows_own = project(token_heads, residual, gain, meta_own, out_weight, slots)
    rows_own = exchange(rows_own)
    _, rows_far = project(heads_far, residual_far, gain, meta_far, out_weight, slots)
    rows_far = exchange(rows_far)
    answer_own = experts_of(rows_own, own, other)
    answer_far = experts_of(rows_far, own, other)
    back_far = exchange(answer_far)
    part_far = partial_sum(meta_far, back_far)
    part = lax.ppermute(part_far, "sp", mirror)
    back_own = exchange(answer_own)
    return final_sum(meta_own, back_own, mixed, part)


def solution(mesh):
    placed = (
        P(("sp", "tp"), None),
        P("sp", "tp"),
        P("sp", "tp"),
        P("sp", "tp"),
        P("tp"),
        P("sp"),
        P(),
        P(),
        P("sp", None, "tp"),
        P("sp", None, "tp"),
        P("sp", "tp", None),
        P(("sp", "tp"), None),
        P(("sp", "tp"), None),
    )
    return jax.shard_map(
        on_device, mesh=mesh, in_specs=placed, out_specs=P(("sp", "tp"), None), check_vma=False
    )
```

```python
import functools

import jax
import jax.numpy as jnp
from jax import lax
from jax.experimental import pallas as pl
from jax.experimental.pallas import tpu as pltpu
from jax.sharding import PartitionSpec as P


HD = 64
REACH = 3
EPS = 1e-06
BF = jnp.bfloat16
F32 = jnp.float32
VM = pl.BlockSpec(memory_space=pltpu.VMEM)
SM = pl.BlockSpec(memory_space=pltpu.SMEM)
ANY = pl.BlockSpec(memory_space=pl.ANY)


def params(mebibytes):
    return pltpu.CompilerParams(vmem_limit_bytes=mebibytes * 1024 * 1024)


def cost(flops, bytes_accessed):
    return pl.CostEstimate(flops=flops, bytes_accessed=bytes_accessed, transcendentals=0)


def pack_kernel(q_ref, k_ref, v_ref, id_ref, o_ref):
    length, width = k_ref.shape
    part = length // 2
    scaled = (q_ref[...].astype(F32) * (HD**-0.5)).astype(BF)
    o_ref[0, :length, :width] = k_ref[...]
    o_ref[0, :length, width:] = v_ref[...]
    o_ref[0, length : length + 16, :] = id_ref[...]
    o_ref[0, length + 16 :, :width] = scaled[:part]
    o_ref[0, length + 16 :, width:] = scaled[part:]


def pack(query_rows, key_rows, value_rows, id_rows, heads):
    length = query_rows.shape[0]
    width = query_rows.shape[1] // heads
    rows = length + 16 + length // 2
    columns = pl.BlockSpec((length, width), lambda h: (0, h))
    return pl.pallas_call(
        pack_kernel,
        grid=(heads,),
        in_specs=[columns] * 3 + [pl.BlockSpec(id_rows.shape, lambda h: (0, 0))],
        out_specs=pl.BlockSpec((1, rows, 2 * width), lambda h: (h, 0, 0)),
        out_shape=jax.ShapeDtypeStruct((heads, rows, 2 * width), BF),
        compiler_params=params(8),
        name="pack",
    )(query_rows, key_rows, value_rows, id_rows)


def attention_kernel(
    lam_ref, prev_ref, own_ref, next_ref, o_ref, k_ref, v_ref, line_ref, id_ref
):
    b = pl.program_id(0)
    length, width = o_ref.shape[1:]
    before, group, after = prev_ref.shape[0], own_ref.shape[0], next_ref.shape[0]
    span = before + 1 + after
    blocks = before + group + after

    @pl.when(b == 0)
    def _():
        id_ref[...] = jnp.zeros_like(id_ref)
        for first, ref in ((0, prev_ref), (before, own_ref), (before + group, next_ref)):
            for i in range(ref.shape[0]):
                rows = slice((first + i) * length, (first + i + 1) * length)
                k_ref[rows, :] = ref[i, :length, :width]
                v_ref[rows, :width] = ref[i, :length, width:]
                named = ref[i, length : length + 16, :].astype(F32)[:1]
                id_ref[first + i : first + i + 1, :] = named
                line_ref[0:1, rows] = named
        v_ref[:, width:] = jnp.ones((v_ref.shape[0], width), BF)
        k_ref[blocks * length :, :] = jnp.zeros((length, width), BF)
        v_ref[blocks * length :, :width] = jnp.zeros((length, width), BF)
        line_ref[0:1, blocks * length :] = jnp.zeros((1, length), F32)

    query_ids = id_ref[pl.ds(b + before, 1), :]
    low = jnp.min(query_ids, axis=1, keepdims=True)
    high = jnp.max(query_ids, axis=1, keepdims=True)
    ids = id_ref[...]
    smallest = jnp.min(ids, axis=1, keepdims=True)
    largest = jnp.max(ids, axis=1, keepdims=True)
    place = lax.broadcasted_iota(jnp.int32, smallest.shape, 0) - b
    apart = (largest < low) | (smallest > high)
    left = jnp.sum(jnp.where(apart & (place >= 0) & (place < before), 1.0, 0.0))
    right = jnp.sum(jnp.where(apart & (place > before) & (place < span), 1.0, 0.0))
    left = left.astype(jnp.int32)
    pairs = (span + 1 - right.astype(jnp.int32) - left) // 2
    start = pl.multiple_of((b + left) * length, length)
    query_column = jnp.transpose(jnp.broadcast_to(query_ids, (128, length)))
    lam = lam_ref[0]

    def attend(keys):
        named = line_ref[0:1, pl.ds(start, keys)]
        for chunk in range(length // 128):
            mine = query_column[chunk * 128 : (chunk + 1) * 128, :]
            q = own_ref[
                b,
                length + 16 + (chunk * 128) % (length // 2) : length
                + 16
                + (chunk * 128) % (length // 2)
                + 128,
                (chunk * 128 // (length // 2)) * width : (chunk * 128 // (length // 2) + 1) * width,
            ]
            zero = jnp.zeros((128, HD), BF)
            sides = (
                jnp.concatenate([q[:, :HD], zero], axis=1),
                jnp.concatenate([zero, q[:, HD:]], axis=1),
            )
            maps = []
            for side in sides:
                scores = lax.dot_general(
                    side,
                    k_ref[pl.ds(start, keys), :],
                    (((1,), (1,)), ((), ())),
                    preferred_element_type=F32,
                )
                pieces = []
                best = None
                for part in range(keys // 128):
                    columns = slice(part * 128, (part + 1) * 128)
                    piece = jnp.where(mine == named[:, columns], scores[:, columns], -1e30)
                    best = piece if best is None else jnp.maximum(best, piece)
                    pieces.append(piece)
                top = jnp.max(best, axis=1, keepdims=True)
                lifted = jnp.concatenate(
                    [jnp.exp(piece - top).astype(BF) for piece in pieces], axis=1
                )
                total = jnp.dot(
                    lifted, v_ref[pl.ds(start, keys), :], preferred_element_type=F32
                )
                maps.append(total[:, :width] / total[:, width:])
            out = maps[0] - lam * maps[1]
            scale = lax.rsqrt(jnp.mean(out * out, axis=1, keepdims=True) + EPS)
            o_ref[b, chunk * 128 : (chunk + 1) * 128, :] = (out * scale).astype(BF)

    for count in range(1, (span + 1) // 2 + 1):

        @pl.when(pairs == count)
        def _():
            attend(count * 2 * length)


def attention(lam, prev, own, following, length, width):
    group = own.shape[0]
    before, after = prev.shape[0], following.shape[0]
    blocks = before + group + after
    return pl.pallas_call(
        attention_kernel,
        grid=(group,),
        in_specs=[SM] + [VM] * 3,
        out_specs=VM,
        out_shape=jax.ShapeDtypeStruct((group, length, width), BF),
        scratch_shapes=[
            pltpu.VMEM(((blocks + 1) * length, width), BF),
            pltpu.VMEM(((blocks + 1) * length, 2 * width), BF),
            pltpu.VMEM((8, (blocks + 1) * length), F32),
            pltpu.VMEM((-(-(blocks + 1) // 8) * 8, length), F32),
        ],
        compiler_params=params(16),
        cost_estimate=cost(8 * 10**9, 4 * 10**6),
        name="attention",
    )(lam, prev, own, following)


def project_kernel(
    heads_ref, residual_ref, gain_ref, meta_ref, weight_ref, rows_ref, mixed_ref, left_ref, *, tile
):
    tokens, width = mixed_ref.shape
    members = heads_ref.shape[0]
    value_dim = heads_ref.shape[2]
    for source in range(members):
        head = (source % 2) * (members // 2) + source // 2
        left_ref[:, head * value_dim : (head + 1) * value_dim] = heads_ref[source]
    squares = jnp.zeros((tokens, 128), F32)
    for n in range(width // tile):
        columns = slice(n * tile, (n + 1) * tile)
        projected = jnp.dot(left_ref[...], weight_ref[:, columns], preferred_element_type=F32)
        mixed = (residual_ref[:, columns].astype(F32) + projected).astype(BF)
        mixed_ref[:, columns] = mixed
        wide = mixed.astype(F32)
        wide = wide * wide
        for part in range(tile // 128):
            squares = squares + wide[:, part * 128 : (part + 1) * 128]
    scale = lax.rsqrt(jnp.sum(squares, axis=1, keepdims=True) / width + EPS)
    slots = rows_ref.shape[0]
    place = lax.broadcasted_iota(jnp.int32, (slots, tokens), 0).astype(F32)
    pick = (place == meta_ref[0:1, :]) | (place == meta_ref[1:2, :])
    pick = jnp.where(pick, 1.0, 0.0).astype(BF)
    for n in range(width // tile):
        columns = slice(n * tile, (n + 1) * tile)
        normed = mixed_ref[:, columns].astype(F32) * scale * gain_ref[:, columns]
        rows_ref[:, columns] = jnp.dot(
            pick, normed.astype(BF), preferred_element_type=F32
        ).astype(BF)


def project(heads, residual, gain, meta, out_weight, slots, keep, tile=512):
    _, tokens, _ = heads.shape
    depth, width = out_weight.shape
    rows = jax.ShapeDtypeStruct((slots, width), BF)
    mixed = jax.ShapeDtypeStruct((tokens, width), BF)
    left = pltpu.VMEM((tokens, depth), BF)
    return pl.pallas_call(
        functools.partial(project_kernel, tile=tile),
        in_specs=[VM] * 5,
        out_specs=[VM, VM] if keep else VM,
        out_shape=[rows, mixed] if keep else rows,
        scratch_shapes=[left] if keep else [pltpu.VMEM((tokens, width), BF), left],
        compiler_params=params(16),
        cost_estimate=cost(3 * 10**9, 8 * 10**6),
    )(heads, residual, gain, meta, out_weight)


def expert_kernel(
    x_ref, g0, u0, d0, g1, u1, d1, y_ref, gb, ub, db, hidden_ref, half_ref, sems, *, tile
):
    steps = g0.shape[1] // tile
    width = y_ref.shape[1]
    arrivals = []
    for step in range(steps):
        at = pl.ds(step * tile, tile)
        arrivals.append(
            (
                pltpu.make_async_copy(g1.at[:, at], gb.at[:, at], sems.at[step]),
                pltpu.make_async_copy(u1.at[:, at], ub.at[:, at], sems.at[steps + step]),
            )
        )
    last = [
        pltpu.make_async_copy(
            d1.at[pl.ds(n * tile, tile)], db.at[pl.ds(n * tile, tile)], sems.at[2 * steps + n]
        )
        for n in range(steps)
    ]
    for pair in arrivals:
        for copy in pair:
            copy.start()
    for copy in last:
        copy.start()
    for h, (g, u, d) in enumerate(((g0, u0, d0), (gb, ub, db))):
        for step in range(steps):
            at = slice(step * tile, (step + 1) * tile)
            if h:
                for copy in arrivals[step]:
                    copy.wait()
            gate = jnp.dot(x_ref[...], g[:, at], preferred_element_type=F32)
            upward = jnp.dot(x_ref[...], u[:, at], preferred_element_type=F32)
            hidden_ref[:, at] = (gate / (1.0 + jnp.exp(-gate)) * upward).astype(BF)
        if h:
            for copy in last:
                copy.wait()
        for n in range(width // tile):
            at = slice(n * tile, (n + 1) * tile)
            part = jnp.dot(hidden_ref[...], d[:, at], preferred_element_type=F32).astype(BF)
            if h:
                y_ref[:, at] = (half_ref[:, at].astype(F32) + part.astype(F32)).astype(BF)
            else:
                half_ref[:, at] = part


def experts_of(x, own, other, tile=256):
    rows, width = x.shape
    depth = own[0].shape[1]
    return pl.pallas_call(
        functools.partial(expert_kernel, tile=tile),
        in_specs=[VM] * 4 + [ANY] * 3,
        out_specs=VM,
        out_shape=jax.ShapeDtypeStruct((rows, width), BF),
        scratch_shapes=[
            pltpu.VMEM((width, depth), BF),
            pltpu.VMEM((width, depth), BF),
            pltpu.VMEM((depth, width), BF),
            pltpu.VMEM((rows, depth), BF),
            pltpu.VMEM((rows, width), BF),
            pltpu.SemaphoreType.DMA((3 * (depth // tile),)),
        ],
        compiler_params=params(34),
        cost_estimate=cost(9 * 10**9, 26 * 10**6),
    )(x, *own, *other)


def picked(meta_ref, rows_ref, write, tile=512):
    slots, width = rows_ref.shape
    tokens = meta_ref.shape[1]
    columns = jnp.transpose(meta_ref[...])
    place = lax.broadcasted_iota(jnp.int32, (tokens, slots), 1).astype(F32)
    picks = jnp.concatenate(
        [jnp.where(place == columns[:, k : k + 1], 1.0, 0.0) for k in range(2)], axis=0
    ).astype(BF)
    for n in range(width // tile):
        at = slice(n * tile, (n + 1) * tile)
        rows = jnp.dot(picks, rows_ref[:, at], preferred_element_type=F32)
        write(at, rows[:tokens] * columns[:, 2:3] + rows[tokens:] * columns[:, 3:4])


def partial_kernel(meta_ref, rows_ref, o_ref):
    def write(at, total):
        o_ref[:, at] = total.astype(BF)

    picked(meta_ref, rows_ref, write)


def final_kernel(meta_ref, rows_ref, mixed_ref, far_ref, o_ref):
    def write(at, total):
        total = total + far_ref[:, at].astype(F32)
        o_ref[:, at] = (mixed_ref[:, at].astype(F32) + total).astype(BF)

    picked(meta_ref, rows_ref, write)


def partial_sum(meta, rows):
    return pl.pallas_call(
        partial_kernel,
        in_specs=[VM] * 2,
        out_specs=VM,
        out_shape=jax.ShapeDtypeStruct((meta.shape[1], rows.shape[1]), BF),
        compiler_params=params(12),
        cost_estimate=cost(10**9, 2 * 10**6),
        name="partial_sum",
    )(meta, rows)


def final_sum(meta, rows, mixed, far):
    return pl.pallas_call(
        final_kernel,
        in_specs=[VM] * 4,
        out_specs=VM,
        out_shape=jax.ShapeDtypeStruct(mixed.shape, BF),
        compiler_params=params(12),
        cost_estimate=cost(10**9, 3 * 10**6),
        name="final_sum",
    )(meta, rows, mixed, far)


def ranks_of(routes, experts):
    tokens = routes.shape[0]
    table = (routes[:, :, None] == jnp.arange(experts, dtype=jnp.int32)).astype(F32)
    named = jnp.sum(table, axis=1)
    order = jnp.arange(tokens)
    below = (order[:, None] > order[None, :]).astype(BF)
    earlier = jnp.dot(below, named.astype(BF), preferred_element_type=F32)
    return jnp.sum(earlier[:, None, :] * table, axis=2)


def meta_of(routes, ranks, route_weights, first, count, capacity):
    local = routes - first
    inside = (local >= 0) & (local < count)
    target = jnp.where(inside, local.astype(F32) * capacity + ranks, -1.0)
    rows = jnp.concatenate([target.T, route_weights.T], axis=0)
    return jnp.concatenate([rows, jnp.zeros((8 - rows.shape[0], rows.shape[1]), F32)], axis=0)


def on_device(
    residual,
    query_rows,
    key_rows,
    value_rows,
    mix_lambda,
    documents,
    out_weight,
    norm_gain,
    gate_weight,
    up_weight,
    down_weight,
    routes,
    route_weights,
):
    length = query_rows.shape[0]
    heads = mix_lambda.shape[0]
    width = residual.shape[1]
    count = lax.axis_size("sp")
    twins = lax.axis_size("tp")
    here = lax.axis_index("sp")
    half = count // 2
    capacity = 2 * length // count
    planes = [[g * heads + j for j in range(heads)] for g in range(count // heads)]
    halves = [[h * half + j for j in range(half)] for h in range(2)]
    mirror = [(i, (i + half) % count) for i in range(count)]
    swap = [(i, twins - 1 - i) for i in range(twins)]

    value_dim = value_rows.shape[1] // heads
    id_rows = jnp.broadcast_to((documents + 1).astype(BF)[None, :], (16, length))
    packed = pack(query_rows, key_rows, value_rows, id_rows, heads)
    packed = lax.all_to_all(packed, "sp", 0, 0, tiled=True, axis_index_groups=planes)
    pairs = packed[:, : length + 16]
    prev = lax.ppermute(
        pairs[heads - REACH :], "sp", [(i, i + heads) for i in range(count - heads)]
    )
    following = lax.ppermute(pairs[:REACH], "sp", [(i + heads, i) for i in range(count - heads)])

    ranks = ranks_of(routes, count)
    my_half = here // half
    meta_own = meta_of(routes, ranks, route_weights, my_half * half, half, capacity)
    meta_far = meta_of(routes, ranks, route_weights, (1 - my_half) * half, half, capacity)
    meta_far = lax.ppermute(meta_far, "sp", mirror)
    prev, following, residual_late = lax.optimization_barrier((prev, following, residual))
    residual_far = lax.ppermute(residual_late, "sp", mirror)

    own = (gate_weight[0], up_weight[0], down_weight[0])
    other = tuple(lax.ppermute(weight, "tp", swap) for weight in own)

    lam = lax.dynamic_slice(mix_lambda, (here % heads,), (1,))
    outs = attention(lam, prev, packed, following, length, value_dim)
    outs = outs.reshape(heads * twins, length // twins, value_dim)
    both = [[g * heads * twins + j for j in range(heads * twins)] for g in range(count // heads)]
    token_heads = lax.all_to_all(
        outs, ("sp", "tp"), 0, 0, tiled=True, axis_index_groups=both
    )
    heads_far = lax.ppermute(token_heads, "sp", mirror)

    gain = norm_gain.reshape(1, width)
    slots = half * capacity

    def exchange(rows):
        rows = rows.reshape(half, capacity, width)
        rows = lax.all_to_all(rows, "sp", 0, 0, tiled=True, axis_index_groups=halves)
        return rows.reshape(slots, width)

    rows_own, mixed = project(token_heads, residual, gain, meta_own, out_weight, slots, True)
    rows_own = exchange(rows_own)
    rows_far = project(heads_far, residual_far, gain, meta_far, out_weight, slots, False)
    rows_far = exchange(rows_far)
    answer_own = experts_of(rows_own, own, other)
    answer_far = experts_of(rows_far, own, other)
    back_far = exchange(answer_far)
    part_far = partial_sum(meta_far, back_far)
    part = lax.ppermute(part_far, "sp", mirror)
    back_own = exchange(answer_own)
    return final_sum(meta_own, back_own, mixed, part)


def solution(mesh):
    placed = (
        P(("sp", "tp"), None),
        P("sp", "tp"),
        P("sp", "tp"),
        P("sp", "tp"),
        P("tp"),
        P("sp"),
        P(),
        P(),
        P("sp", None, "tp"),
        P("sp", None, "tp"),
        P("sp", "tp", None),
        P(("sp", "tp"), None),
        P(("sp", "tp"), None),
    )
    return jax.shard_map(
        on_device, mesh=mesh, in_specs=placed, out_specs=P(("sp", "tp"), None), check_vma=False
    )
```

```python
import functools

import jax
import jax.numpy as jnp
from jax import lax
from jax.experimental import pallas as pl
from jax.experimental.pallas import tpu as pltpu
from jax.sharding import PartitionSpec as P


HD = 64
REACH = 3
EPS = 1e-06
BF = jnp.bfloat16
F32 = jnp.float32
VM = pl.BlockSpec(memory_space=pltpu.VMEM)
SM = pl.BlockSpec(memory_space=pltpu.SMEM)
ANY = pl.BlockSpec(memory_space=pl.ANY)


def params(mebibytes):
    return pltpu.CompilerParams(vmem_limit_bytes=mebibytes * 1024 * 1024)


def in_hbm(value):
    return pltpu.with_memory_space_constraint(value, pltpu.HBM)


def cost(flops, bytes_accessed):
    return pl.CostEstimate(flops=flops, bytes_accessed=bytes_accessed, transcendentals=0)


def pack_kernel(q_ref, k_ref, v_ref, id_ref, o_ref):
    length, width = k_ref.shape
    part = length // 2
    scaled = (q_ref[...].astype(F32) * (HD**-0.5)).astype(BF)
    o_ref[0, :length, :width] = k_ref[...]
    o_ref[0, :length, width:] = v_ref[...]
    o_ref[0, length : length + 16, :] = id_ref[...]
    o_ref[0, length + 16 :, :width] = scaled[:part]
    o_ref[0, length + 16 :, width:] = scaled[part:]


def pack(query_rows, key_rows, value_rows, id_rows, heads):
    length = query_rows.shape[0]
    width = query_rows.shape[1] // heads
    rows = length + 16 + length // 2
    columns = pl.BlockSpec((length, width), lambda h: (0, h))
    return pl.pallas_call(
        pack_kernel,
        grid=(heads,),
        in_specs=[columns] * 3 + [pl.BlockSpec(id_rows.shape, lambda h: (0, 0))],
        out_specs=pl.BlockSpec((1, rows, 2 * width), lambda h: (h, 0, 0)),
        out_shape=jax.ShapeDtypeStruct((heads, rows, 2 * width), BF),
        compiler_params=params(8),
        name="pack",
    )(*(in_hbm(rows) for rows in (query_rows, key_rows, value_rows)), id_rows)


def attention_kernel(
    lam_ref,
    prev_ref,
    own_ref,
    next_ref,
    o_ref,
    k_ref,
    v_ref,
    line_ref,
    id_ref,
):
    b = pl.program_id(0)
    length, width = o_ref.shape[1:]
    before, group, after = prev_ref.shape[0], own_ref.shape[0], next_ref.shape[0]
    span = before + 1 + after
    blocks = before + group + after

    @pl.when(b == 0)
    def _():
        id_ref[...] = jnp.zeros_like(id_ref)
        for first, ref in ((0, prev_ref), (before, own_ref), (before + group, next_ref)):
            for i in range(ref.shape[0]):
                rows = slice((first + i) * length, (first + i + 1) * length)
                k_ref[rows, :] = ref[i, :length, :width]
                v_ref[rows, :width] = ref[i, :length, width:]
                named = ref[i, length : length + 16, :].astype(F32)[:1]
                id_ref[first + i : first + i + 1, :] = named
                line_ref[0:1, rows] = named
        v_ref[:, width:] = jnp.ones((v_ref.shape[0], width), BF)
        k_ref[blocks * length :, :] = jnp.zeros((length, width), BF)
        v_ref[blocks * length :, :width] = jnp.zeros((length, width), BF)
        line_ref[0:1, blocks * length :] = jnp.zeros((1, length), F32)

    query_ids = id_ref[pl.ds(b + before, 1), :]
    low = jnp.min(query_ids, axis=1, keepdims=True)
    high = jnp.max(query_ids, axis=1, keepdims=True)
    ids = id_ref[...]
    smallest = jnp.min(ids, axis=1, keepdims=True)
    largest = jnp.max(ids, axis=1, keepdims=True)
    place = lax.broadcasted_iota(jnp.int32, smallest.shape, 0) - b
    apart = (largest < low) | (smallest > high)
    left = jnp.sum(jnp.where(apart & (place >= 0) & (place < before), 1.0, 0.0))
    right = jnp.sum(jnp.where(apart & (place > before) & (place < span), 1.0, 0.0))
    left = left.astype(jnp.int32)
    pairs = (span + 1 - right.astype(jnp.int32) - left) // 2
    start = pl.multiple_of((b + left) * length, length)
    query_column = jnp.transpose(jnp.broadcast_to(query_ids, (128, length)))
    lam = lam_ref[0]

    def attend(keys):
        named = line_ref[0:1, pl.ds(start, keys)]
        for chunk in range(length // 128):
            mine = query_column[chunk * 128 : (chunk + 1) * 128, :]
            q = own_ref[
                b,
                length + 16 + (chunk * 128) % (length // 2) : length
                + 16
                + (chunk * 128) % (length // 2)
                + 128,
                (chunk * 128 // (length // 2)) * width : (chunk * 128 // (length // 2) + 1) * width,
            ]
            zero = jnp.zeros((128, HD), BF)
            sides = (
                jnp.concatenate([q[:, :HD], zero], axis=1),
                jnp.concatenate([zero, q[:, HD:]], axis=1),
            )
            maps = []
            for side in sides:
                scores = lax.dot_general(
                    side,
                    k_ref[pl.ds(start, keys), :],
                    (((1,), (1,)), ((), ())),
                    preferred_element_type=F32,
                )
                pieces = []
                best = None
                for part in range(keys // 128):
                    columns = slice(part * 128, (part + 1) * 128)
                    piece = jnp.where(mine == named[:, columns], scores[:, columns], -1e30)
                    best = piece if best is None else jnp.maximum(best, piece)
                    pieces.append(piece)
                top = jnp.max(best, axis=1, keepdims=True)
                lifted = jnp.concatenate(
                    [jnp.exp(piece - top).astype(BF) for piece in pieces], axis=1
                )
                total = jnp.dot(
                    lifted, v_ref[pl.ds(start, keys), :], preferred_element_type=F32
                )
                maps.append(total[:, :width] / total[:, width:])
            out = maps[0] - lam * maps[1]
            scale = lax.rsqrt(jnp.mean(out * out, axis=1, keepdims=True) + EPS)
            o_ref[b, chunk * 128 : (chunk + 1) * 128, :] = (out * scale).astype(BF)

    for count in range(1, (span + 1) // 2 + 1):

        @pl.when(pairs == count)
        def _():
            attend(count * 2 * length)


def attention(lam, prev, own, following, length, width):
    group = own.shape[0]
    before, after = prev.shape[0], following.shape[0]
    blocks = before + group + after
    return pl.pallas_call(
        attention_kernel,
        grid=(group,),
        in_specs=[SM] + [VM] * 3,
        out_specs=VM,
        out_shape=jax.ShapeDtypeStruct((group, length, width), BF),
        scratch_shapes=[
            pltpu.VMEM(((blocks + 1) * length, width), BF),
            pltpu.VMEM(((blocks + 1) * length, 2 * width), BF),
            pltpu.VMEM((8, (blocks + 1) * length), F32),
            pltpu.VMEM((-(-(blocks + 1) // 8) * 8, length), F32),
        ],
        compiler_params=params(16),
        cost_estimate=cost(8 * 10**9, 4 * 10**6),
        name="attention",
    )(lam, prev, own, following)


def project_kernel(
    heads_ref,
    residual_ref,
    gain_ref,
    meta_ref,
    weight_ref,
    rows_ref,
    mixed_ref,
    left_ref,
    held_ref,
    sems,
    *,
    tile,
):
    tokens, width = mixed_ref.shape
    arrivals = []
    for n in range(width // tile):
        at = pl.ds(n * tile, tile)
        arrivals.append(
            pltpu.make_async_copy(weight_ref.at[:, at], held_ref.at[:, at], sems.at[n])
        )
        arrivals[n].start()
    members = heads_ref.shape[0]
    value_dim = heads_ref.shape[2]
    for source in range(members):
        head = (source % 2) * (members // 2) + source // 2
        left_ref[:, head * value_dim : (head + 1) * value_dim] = heads_ref[source]
    squares = jnp.zeros((tokens, 128), F32)
    for n in range(width // tile):
        columns = slice(n * tile, (n + 1) * tile)
        arrivals[n].wait()
        projected = jnp.dot(left_ref[...], held_ref[:, columns], preferred_element_type=F32)
        mixed = (residual_ref[:, columns].astype(F32) + projected).astype(BF)
        mixed_ref[:, columns] = mixed
        wide = mixed.astype(F32)
        wide = wide * wide
        for part in range(tile // 128):
            squares = squares + wide[:, part * 128 : (part + 1) * 128]
    scale = lax.rsqrt(jnp.sum(squares, axis=1, keepdims=True) / width + EPS)
    slots = rows_ref.shape[0]
    place = lax.broadcasted_iota(jnp.int32, (slots, tokens), 0).astype(F32)
    pick = (place == meta_ref[0:1, :]) | (place == meta_ref[1:2, :])
    pick = jnp.where(pick, 1.0, 0.0).astype(BF)
    for n in range(width // tile):
        columns = slice(n * tile, (n + 1) * tile)
        normed = mixed_ref[:, columns].astype(F32) * scale * gain_ref[:, columns]
        rows_ref[:, columns] = jnp.dot(
            pick, normed.astype(BF), preferred_element_type=F32
        ).astype(BF)


def project(heads, residual, gain, meta, out_weight, slots, keep, tile=512):
    _, tokens, _ = heads.shape
    depth, width = out_weight.shape
    rows = jax.ShapeDtypeStruct((slots, width), BF)
    mixed = jax.ShapeDtypeStruct((tokens, width), BF)
    scratch = [
        pltpu.VMEM((tokens, depth), BF),
        pltpu.VMEM((depth, width), BF),
        pltpu.SemaphoreType.DMA((width // tile,)),
    ]
    return pl.pallas_call(
        functools.partial(project_kernel, tile=tile),
        in_specs=[VM] * 4 + [ANY],
        out_specs=[VM, VM] if keep else VM,
        out_shape=[rows, mixed] if keep else rows,
        scratch_shapes=scratch if keep else [pltpu.VMEM((tokens, width), BF), *scratch],
        compiler_params=params(16),
        cost_estimate=cost(3 * 10**9, 8 * 10**6),
    )(heads, residual, gain, meta, in_hbm(out_weight))


def expert_rows(x_ref, g, u, d, y_ref, hidden_ref, half_ref, tile, arrive):
    halves, width, depth = g.shape
    for h in range(halves):
        for step in range(depth // tile):
            at = slice(step * tile, (step + 1) * tile)
            arrive(h, step)
            gate = jnp.dot(x_ref[...], g[h, :, at], preferred_element_type=F32)
            upward = jnp.dot(x_ref[...], u[h, :, at], preferred_element_type=F32)
            hidden_ref[:, at] = (gate / (1.0 + jnp.exp(-gate)) * upward).astype(BF)
        arrive(h, depth // tile)
        for n in range(width // tile):
            at = slice(n * tile, (n + 1) * tile)
            part = jnp.dot(hidden_ref[...], d[h, :, at], preferred_element_type=F32).astype(BF)
            if h:
                y_ref[:, at] = (half_ref[:, at].astype(F32) + part.astype(F32)).astype(BF)
            else:
                half_ref[:, at] = part


def expert_kernel(
    x_ref, g0, u0, d0, g1, u1, d1, y_ref, gs, us, ds, hidden_ref, half_ref, sems, *, tile
):
    steps = g0.shape[1] // tile
    arrivals = []
    for h, (g, u, d) in enumerate(((g0, u0, d0), (g1, u1, d1))):
        waves = []
        for step in range(steps):
            at = pl.ds(step * tile, tile)
            waves.append(
                (
                    pltpu.make_async_copy(g.at[:, at], gs.at[h, :, at], sems.at[h, 2 * step]),
                    pltpu.make_async_copy(u.at[:, at], us.at[h, :, at], sems.at[h, 2 * step + 1]),
                )
            )
        waves.append((pltpu.make_async_copy(d, ds.at[h], sems.at[h, 2 * steps]),))
        arrivals.append(waves)
    for waves in arrivals:
        for wave in waves:
            for copy in wave:
                copy.start()

    def arrive(h, step):
        for copy in arrivals[h][step]:
            copy.wait()

    expert_rows(x_ref, gs, us, ds, y_ref, hidden_ref, half_ref, tile, arrive)


def experts_of(x, own, other, tile=256):
    rows, width = x.shape
    depth = own[0].shape[1]
    return pl.pallas_call(
        functools.partial(expert_kernel, tile=tile),
        in_specs=[VM] + [ANY] * 6,
        out_specs=VM,
        out_shape=jax.ShapeDtypeStruct((rows, width), BF),
        scratch_shapes=[
            pltpu.VMEM((2, width, depth), BF),
            pltpu.VMEM((2, width, depth), BF),
            pltpu.VMEM((2, depth, width), BF),
            pltpu.VMEM((rows, depth), BF),
            pltpu.VMEM((rows, width), BF),
            pltpu.SemaphoreType.DMA((2, 2 * (depth // tile) + 1)),
        ],
        compiler_params=params(40),
        cost_estimate=cost(9 * 10**9, 26 * 10**6),
    )(x, *(in_hbm(weight) for weight in (*own, *other)))


def picked(meta_ref, rows_ref, write, tile=512):
    slots, width = rows_ref.shape
    tokens = meta_ref.shape[1]
    columns = jnp.transpose(meta_ref[...])
    place = lax.broadcasted_iota(jnp.int32, (tokens, slots), 1).astype(F32)
    picks = jnp.concatenate(
        [jnp.where(place == columns[:, k : k + 1], 1.0, 0.0) for k in range(2)], axis=0
    ).astype(BF)
    for n in range(width // tile):
        at = slice(n * tile, (n + 1) * tile)
        rows = jnp.dot(picks, rows_ref[:, at], preferred_element_type=F32)
        write(at, rows[:tokens] * columns[:, 2:3] + rows[tokens:] * columns[:, 3:4])


def partial_kernel(meta_ref, rows_ref, o_ref):
    def write(at, total):
        o_ref[:, at] = total.astype(BF)

    picked(meta_ref, rows_ref, write)


def final_kernel(meta_ref, rows_ref, mixed_ref, far_ref, o_ref):
    def write(at, total):
        total = total + far_ref[:, at].astype(F32)
        o_ref[:, at] = (mixed_ref[:, at].astype(F32) + total).astype(BF)

    picked(meta_ref, rows_ref, write)


def partial_sum(meta, rows):
    return pl.pallas_call(
        partial_kernel,
        in_specs=[VM] * 2,
        out_specs=VM,
        out_shape=jax.ShapeDtypeStruct((meta.shape[1], rows.shape[1]), BF),
        compiler_params=params(12),
        cost_estimate=cost(10**9, 2 * 10**6),
        name="partial_sum",
    )(meta, rows)


def final_sum(meta, rows, mixed, far):
    return pl.pallas_call(
        final_kernel,
        in_specs=[VM] * 4,
        out_specs=VM,
        out_shape=jax.ShapeDtypeStruct(mixed.shape, BF),
        compiler_params=params(12),
        cost_estimate=cost(10**9, 3 * 10**6),
        name="final_sum",
    )(meta, rows, mixed, far)


def ranks_of(routes, experts):
    tokens = routes.shape[0]
    table = (routes[:, :, None] == jnp.arange(experts, dtype=jnp.int32)).astype(F32)
    named = jnp.sum(table, axis=1)
    order = jnp.arange(tokens)
    below = (order[:, None] > order[None, :]).astype(BF)
    earlier = jnp.dot(below, named.astype(BF), preferred_element_type=F32)
    return jnp.sum(earlier[:, None, :] * table, axis=2)


def meta_of(routes, ranks, route_weights, first, count, capacity):
    local = routes - first
    inside = (local >= 0) & (local < count)
    target = jnp.where(inside, local.astype(F32) * capacity + ranks, -1.0)
    rows = jnp.concatenate([target.T, route_weights.T], axis=0)
    return jnp.concatenate([rows, jnp.zeros((8 - rows.shape[0], rows.shape[1]), F32)], axis=0)


def on_device(
    residual,
    query_rows,
    key_rows,
    value_rows,
    mix_lambda,
    documents,
    out_weight,
    norm_gain,
    gate_weight,
    up_weight,
    down_weight,
    routes,
    route_weights,
):
    length = query_rows.shape[0]
    heads = mix_lambda.shape[0]
    width = residual.shape[1]
    count = lax.axis_size("sp")
    twins = lax.axis_size("tp")
    here = lax.axis_index("sp")
    half = count // 2
    capacity = 2 * length // count
    planes = [[g * heads + j for j in range(heads)] for g in range(count // heads)]
    halves = [[h * half + j for j in range(half)] for h in range(2)]
    mirror = [(i, i ^ (count - count // 4)) for i in range(count)]
    swap = [(i, twins - 1 - i) for i in range(twins)]

    value_dim = value_rows.shape[1] // heads
    id_rows = jnp.broadcast_to((documents + 1).astype(BF)[None, :], (16, length))
    packed = pack(query_rows, key_rows, value_rows, id_rows, heads)
    packed = lax.all_to_all(packed, "sp", 0, 0, tiled=True, axis_index_groups=planes)
    pairs = packed[:, : length + 16]
    prev = lax.ppermute(
        pairs[heads - REACH :], "sp", [(i, i + heads) for i in range(count - heads)]
    )
    following = lax.ppermute(pairs[:REACH], "sp", [(i + heads, i) for i in range(count - heads)])

    ranks = ranks_of(routes, count)
    my_half = here // half
    meta_own = meta_of(routes, ranks, route_weights, my_half * half, half, capacity)
    meta_far = meta_of(routes, ranks, route_weights, (1 - my_half) * half, half, capacity)
    meta_far = lax.ppermute(meta_far, "sp", mirror)
    prev, following, residual_late = lax.optimization_barrier((prev, following, residual))
    residual_far = lax.ppermute(residual_late, "sp", mirror)

    own = (gate_weight[0], up_weight[0], down_weight[0])
    other = tuple(lax.ppermute(weight, "tp", swap) for weight in own)

    lam = lax.dynamic_slice(mix_lambda, (here % heads,), (1,))
    outs = attention(lam, prev, packed, following, length, value_dim)
    outs = outs.reshape(heads * twins, length // twins, value_dim)
    both = [[g * heads * twins + j for j in range(heads * twins)] for g in range(count // heads)]
    token_heads = lax.all_to_all(
        outs, ("sp", "tp"), 0, 0, tiled=True, axis_index_groups=both
    )
    heads_far = lax.ppermute(token_heads, "sp", mirror)

    gain = norm_gain.reshape(1, width)
    slots = half * capacity

    def exchange(rows):
        rows = rows.reshape(half, capacity, width)
        rows = lax.all_to_all(rows, "sp", 0, 0, tiled=True, axis_index_groups=halves)
        return rows.reshape(slots, width)

    rows_own, mixed = project(token_heads, residual, gain, meta_own, out_weight, slots, True)
    rows_own = exchange(rows_own)
    rows_far = project(heads_far, residual_far, gain, meta_far, out_weight, slots, False)
    rows_far = exchange(rows_far)
    answer_own = experts_of(rows_own, own, other)
    answer_far = experts_of(rows_far, own, other)
    back_far = exchange(answer_far)
    part_far = partial_sum(meta_far, back_far)
    part = lax.ppermute(part_far, "sp", mirror)
    back_own = exchange(answer_own)
    return final_sum(meta_own, back_own, mixed, part)


def solution(mesh):
    placed = (
        P(("sp", "tp"), None),
        P("sp", "tp"),
        P("sp", "tp"),
        P("sp", "tp"),
        P("tp"),
        P("sp"),
        P(),
        P(),
        P("sp", None, "tp"),
        P("sp", None, "tp"),
        P("sp", "tp", None),
        P(("sp", "tp"), None),
        P(("sp", "tp"), None),
    )
    return jax.shard_map(
        on_device, mesh=mesh, in_specs=placed, out_specs=P(("sp", "tp"), None), check_vma=False
    )
```

```python
import functools

import jax
import jax.numpy as jnp
from jax import lax
from jax.experimental import pallas as pl
from jax.experimental.pallas import tpu as pltpu
from jax.sharding import PartitionSpec as P


HD = 64
REACH = 3
EPS = 1e-06
BF = jnp.bfloat16
F32 = jnp.float32
VM = pl.BlockSpec(memory_space=pltpu.VMEM)
SM = pl.BlockSpec(memory_space=pltpu.SMEM)
ANY = pl.BlockSpec(memory_space=pl.ANY)


def params(mebibytes):
    return pltpu.CompilerParams(vmem_limit_bytes=mebibytes * 1024 * 1024)


def in_hbm(value):
    return pltpu.with_memory_space_constraint(value, pltpu.HBM)


def cost(flops, bytes_accessed):
    return pl.CostEstimate(flops=flops, bytes_accessed=bytes_accessed, transcendentals=0)


def pack_kernel(k_ref, v_ref, id_ref, o_ref):
    heads, _, width = o_ref.shape
    length = k_ref.shape[0]
    part = width // 2
    for h in range(heads):
        columns = slice(h * part, (h + 1) * part)
        o_ref[h, :length, :part] = k_ref[:, columns]
        o_ref[h, :length, part:] = v_ref[:, columns]
        o_ref[h, length:, :] = id_ref[...]


def pack(key_rows, value_rows, id_rows, heads):
    length = key_rows.shape[0]
    width = key_rows.shape[1] // heads
    return pl.pallas_call(
        pack_kernel,
        in_specs=[VM] * 3,
        out_specs=VM,
        out_shape=jax.ShapeDtypeStruct((heads, length + 16, 2 * width), BF),
        compiler_params=params(8),
        name="pack",
    )(in_hbm(key_rows), in_hbm(value_rows), id_rows)


def attention_kernel(
    lam_ref,
    q_ref,
    prev_ref,
    own_ref,
    next_ref,
    o_ref,
    k_ref,
    v_ref,
    line_ref,
    id_ref,
    bound_ref,
):
    b = pl.program_id(0)
    length, width = o_ref.shape[1:]
    before, group, after = prev_ref.shape[0], own_ref.shape[0], next_ref.shape[0]
    span = before + 1 + after
    blocks = before + group + after

    @pl.when(b == 0)
    def _():
        id_ref[...] = jnp.zeros_like(id_ref)
        for first, ref in ((0, prev_ref), (before, own_ref), (before + group, next_ref)):
            for i in range(ref.shape[0]):
                rows = slice((first + i) * length, (first + i + 1) * length)
                k_ref[rows, :] = ref[i, :length, :width]
                v_ref[rows, :width] = ref[i, :length, width:]
                named = ref[i, length : length + 16, :].astype(F32)[:1]
                id_ref[first + i : first + i + 1, :] = named
                line_ref[0:1, rows] = named
        v_ref[:, width:] = jnp.ones((v_ref.shape[0], width), BF)
        k_ref[blocks * length :, :] = jnp.zeros((length, width), BF)
        v_ref[blocks * length :, :width] = jnp.zeros((length, width), BF)
        line_ref[0:1, blocks * length :] = jnp.zeros((1, length), F32)

        ids = id_ref[...]
        smallest = jnp.min(ids, axis=1, keepdims=True)
        largest = jnp.max(ids, axis=1, keepdims=True)
        place = lax.broadcasted_iota(jnp.int32, smallest.shape, 0)
        for i in range(group):
            low = smallest[before + i : before + i + 1]
            high = largest[before + i : before + i + 1]
            apart = (largest < low) | (smallest > high)
            early = apart & (place >= i) & (place < i + before)
            late = apart & (place > i + before) & (place < i + span)
            bound_ref[0, i] = jnp.sum(jnp.where(early, 1.0, 0.0)).astype(jnp.int32)
            bound_ref[1, i] = jnp.sum(jnp.where(late, 1.0, 0.0)).astype(jnp.int32)

    query_ids = id_ref[pl.ds(b + before, 1), :]
    left = bound_ref[0, b]
    pairs = (span + 1 - bound_ref[1, b] - left) // 2
    start = pl.multiple_of((b + left) * length, length)
    query_column = jnp.transpose(jnp.broadcast_to(query_ids, (128, length)))
    lam = lam_ref[0]

    def attend(keys):
        named = line_ref[0:1, pl.ds(start, keys)]
        for chunk in range(length // 128):
            mine = query_column[chunk * 128 : (chunk + 1) * 128, :]
            q = q_ref[b, chunk * 128 : (chunk + 1) * 128, :]
            q = (q.astype(F32) * (HD**-0.5)).astype(BF)
            zero = jnp.zeros((128, HD), BF)
            sides = (
                jnp.concatenate([q[:, :HD], zero], axis=1),
                jnp.concatenate([zero, q[:, HD:]], axis=1),
            )
            maps = []
            for side in sides:
                scores = lax.dot_general(
                    side,
                    k_ref[pl.ds(start, keys), :],
                    (((1,), (1,)), ((), ())),
                    preferred_element_type=F32,
                )
                pieces = []
                best = None
                for part in range(keys // 128):
                    columns = slice(part * 128, (part + 1) * 128)
                    piece = jnp.where(mine == named[:, columns], scores[:, columns], -1e30)
                    best = piece if best is None else jnp.maximum(best, piece)
                    pieces.append(piece)
                top = jnp.max(best, axis=1, keepdims=True)
                lifted = jnp.concatenate(
                    [jnp.exp(piece - top).astype(BF) for piece in pieces], axis=1
                )
                total = jnp.dot(
                    lifted, v_ref[pl.ds(start, keys), :], preferred_element_type=F32
                )
                maps.append(total[:, :width] / total[:, width:])
            out = maps[0] - lam * maps[1]
            scale = lax.rsqrt(jnp.mean(out * out, axis=1, keepdims=True) + EPS)
            o_ref[b, chunk * 128 : (chunk + 1) * 128, :] = (out * scale).astype(BF)

    for count in range(1, (span + 1) // 2 + 1):

        @pl.when(pairs == count)
        def _():
            attend(count * 2 * length)


def attention(lam, queries, prev, own, following):
    group, length, width = queries.shape
    before, after = prev.shape[0], following.shape[0]
    blocks = before + group + after
    return pl.pallas_call(
        attention_kernel,
        grid=(group,),
        in_specs=[SM] + [VM] * 4,
        out_specs=VM,
        out_shape=jax.ShapeDtypeStruct((group, length, width), BF),
        scratch_shapes=[
            pltpu.VMEM(((blocks + 1) * length, width), BF),
            pltpu.VMEM(((blocks + 1) * length, 2 * width), BF),
            pltpu.VMEM((8, (blocks + 1) * length), F32),
            pltpu.VMEM((-(-(blocks + 1) // 8) * 8, length), F32),
            pltpu.SMEM((2, group), jnp.int32),
        ],
        compiler_params=params(16),
        cost_estimate=cost(8 * 10**9, 4 * 10**6),
        name="attention",
    )(lam, queries, prev, own, following)


def project_kernel(
    heads_ref,
    residual_ref,
    gain_ref,
    meta_ref,
    weight_ref,
    rows_ref,
    mixed_ref,
    left_ref,
    held_ref,
    sems,
    *,
    tile,
):
    tokens, width = mixed_ref.shape
    arrivals = []
    for n in range(width // tile):
        at = pl.ds(n * tile, tile)
        arrivals.append(
            pltpu.make_async_copy(weight_ref.at[:, at], held_ref.at[:, at], sems.at[n])
        )
        arrivals[n].start()
    members = heads_ref.shape[0]
    value_dim = heads_ref.shape[2]
    for source in range(members):
        head = (source % 2) * (members // 2) + source // 2
        left_ref[:, head * value_dim : (head + 1) * value_dim] = heads_ref[source]
    squares = jnp.zeros((tokens, 128), F32)
    for n in range(width // tile):
        columns = slice(n * tile, (n + 1) * tile)
        arrivals[n].wait()
        projected = jnp.dot(left_ref[...], held_ref[:, columns], preferred_element_type=F32)
        mixed = (residual_ref[:, columns].astype(F32) + projected).astype(BF)
        mixed_ref[:, columns] = mixed
        wide = mixed.astype(F32)
        wide = wide * wide
        for part in range(tile // 128):
            squares = squares + wide[:, part * 128 : (part + 1) * 128]
    scale = lax.rsqrt(jnp.sum(squares, axis=1, keepdims=True) / width + EPS)
    slots = rows_ref.shape[0]
    place = lax.broadcasted_iota(jnp.int32, (slots, tokens), 0).astype(F32)
    pick = (place == meta_ref[0:1, :]) | (place == meta_ref[1:2, :])
    pick = jnp.where(pick, 1.0, 0.0).astype(BF)
    for n in range(width // tile):
        columns = slice(n * tile, (n + 1) * tile)
        normed = mixed_ref[:, columns].astype(F32) * scale * gain_ref[:, columns]
        rows_ref[:, columns] = jnp.dot(
            pick, normed.astype(BF), preferred_element_type=F32
        ).astype(BF)


def project(heads, residual, gain, meta, out_weight, slots, keep, tile=512):
    _, tokens, _ = heads.shape
    depth, width = out_weight.shape
    rows = jax.ShapeDtypeStruct((slots, width), BF)
    mixed = pltpu.HBM((tokens, width), BF)
    scratch = [
        pltpu.VMEM((tokens, depth), BF),
        pltpu.VMEM((depth, width), BF),
        pltpu.SemaphoreType.DMA((width // tile,)),
    ]
    return pl.pallas_call(
        functools.partial(project_kernel, tile=tile),
        in_specs=[VM] * 4 + [ANY],
        out_specs=[VM, VM] if keep else VM,
        out_shape=[rows, mixed] if keep else rows,
        scratch_shapes=scratch if keep else [pltpu.VMEM((tokens, width), BF), *scratch],
        compiler_params=params(16),
        cost_estimate=cost(3 * 10**9, 8 * 10**6),
    )(heads, residual, gain, meta, in_hbm(out_weight))


def expert_rows(x_ref, g, u, d, y_ref, hidden_ref, half_ref, tile, arrive):
    halves, width, depth = g.shape
    for h in range(halves):
        for step in range(depth // tile):
            at = slice(step * tile, (step + 1) * tile)
            arrive(h, step)
            gate = jnp.dot(x_ref[...], g[h, :, at], preferred_element_type=F32)
            upward = jnp.dot(x_ref[...], u[h, :, at], preferred_element_type=F32)
            hidden_ref[:, at] = (gate / (1.0 + jnp.exp(-gate)) * upward).astype(BF)
        arrive(h, depth // tile)
        for n in range(width // tile):
            at = slice(n * tile, (n + 1) * tile)
            part = jnp.dot(hidden_ref[...], d[h, :, at], preferred_element_type=F32).astype(BF)
            if h:
                y_ref[:, at] = (half_ref[:, at].astype(F32) + part.astype(F32)).astype(BF)
            else:
                half_ref[:, at] = part


def expert_kernel(
    x_ref, g0, u0, d0, g1, u1, d1, y_ref, gs, us, ds, hidden_ref, half_ref, sems, *, tile
):
    steps = g0.shape[1] // tile
    arrivals = []
    for h, (g, u, d) in enumerate(((g0, u0, d0), (g1, u1, d1))):
        waves = []
        for step in range(steps):
            at = pl.ds(step * tile, tile)
            waves.append(
                (
                    pltpu.make_async_copy(g.at[:, at], gs.at[h, :, at], sems.at[h, 2 * step]),
                    pltpu.make_async_copy(u.at[:, at], us.at[h, :, at], sems.at[h, 2 * step + 1]),
                )
            )
        waves.append((pltpu.make_async_copy(d, ds.at[h], sems.at[h, 2 * steps]),))
        arrivals.append(waves)
    for waves in arrivals:
        for wave in waves:
            for copy in wave:
                copy.start()

    def arrive(h, step):
        for copy in arrivals[h][step]:
            copy.wait()

    expert_rows(x_ref, gs, us, ds, y_ref, hidden_ref, half_ref, tile, arrive)


def experts_of(x, own, other, tile=256):
    rows, width = x.shape
    depth = own[0].shape[1]
    return pl.pallas_call(
        functools.partial(expert_kernel, tile=tile),
        in_specs=[VM] + [ANY] * 6,
        out_specs=VM,
        out_shape=jax.ShapeDtypeStruct((rows, width), BF),
        scratch_shapes=[
            pltpu.VMEM((2, width, depth), BF),
            pltpu.VMEM((2, width, depth), BF),
            pltpu.VMEM((2, depth, width), BF),
            pltpu.VMEM((rows, depth), BF),
            pltpu.VMEM((rows, width), BF),
            pltpu.SemaphoreType.DMA((2, 2 * (depth // tile) + 1)),
        ],
        compiler_params=params(40),
        cost_estimate=cost(9 * 10**9, 26 * 10**6),
    )(x, *(in_hbm(weight) for weight in (*own, *other)))


def picked(meta_ref, rows_ref, write, tile=512):
    slots, width = rows_ref.shape
    tokens = meta_ref.shape[1]
    columns = jnp.transpose(meta_ref[...])
    place = lax.broadcasted_iota(jnp.int32, (tokens, slots), 1).astype(F32)
    picks = jnp.concatenate(
        [jnp.where(place == columns[:, k : k + 1], 1.0, 0.0) for k in range(2)], axis=0
    ).astype(BF)
    for n in range(width // tile):
        at = slice(n * tile, (n + 1) * tile)
        rows = jnp.dot(picks, rows_ref[:, at], preferred_element_type=F32)
        write(at, rows[:tokens] * columns[:, 2:3] + rows[tokens:] * columns[:, 3:4])


def partial_kernel(meta_ref, rows_ref, o_ref):
    def write(at, total):
        o_ref[:, at] = total.astype(BF)

    picked(meta_ref, rows_ref, write)


def final_kernel(meta_ref, rows_ref, mixed_ref, far_ref, o_ref):
    def write(at, total):
        total = total + far_ref[:, at].astype(F32)
        o_ref[:, at] = (mixed_ref[:, at].astype(F32) + total).astype(BF)

    picked(meta_ref, rows_ref, write)


def partial_sum(meta, rows):
    return pl.pallas_call(
        partial_kernel,
        in_specs=[VM] * 2,
        out_specs=VM,
        out_shape=jax.ShapeDtypeStruct((meta.shape[1], rows.shape[1]), BF),
        compiler_params=params(12),
        cost_estimate=cost(10**9, 2 * 10**6),
        name="partial_sum",
    )(meta, rows)


def final_sum(meta, rows, mixed, far):
    return pl.pallas_call(
        final_kernel,
        in_specs=[VM] * 4,
        out_specs=VM,
        out_shape=jax.ShapeDtypeStruct(mixed.shape, BF),
        compiler_params=params(12),
        cost_estimate=cost(10**9, 3 * 10**6),
        name="final_sum",
    )(meta, rows, mixed, far)


def ranks_of(routes, experts):
    tokens = routes.shape[0]
    table = (routes[:, :, None] == jnp.arange(experts, dtype=jnp.int32)).astype(F32)
    named = jnp.sum(table, axis=1)
    order = jnp.arange(tokens)
    below = (order[:, None] > order[None, :]).astype(BF)
    earlier = jnp.dot(below, named.astype(BF), preferred_element_type=F32)
    return jnp.sum(earlier[:, None, :] * table, axis=2)


def meta_of(routes, ranks, route_weights, first, count, capacity):
    local = routes - first
    inside = (local >= 0) & (local < count)
    target = jnp.where(inside, local.astype(F32) * capacity + ranks, -1.0)
    rows = jnp.concatenate([target.T, route_weights.T], axis=0)
    return jnp.concatenate([rows, jnp.zeros((8 - rows.shape[0], rows.shape[1]), F32)], axis=0)


def on_device(
    residual,
    query_rows,
    key_rows,
    value_rows,
    mix_lambda,
    documents,
    out_weight,
    norm_gain,
    gate_weight,
    up_weight,
    down_weight,
    routes,
    route_weights,
):
    length = query_rows.shape[0]
    heads = mix_lambda.shape[0]
    width = residual.shape[1]
    count = lax.axis_size("sp")
    twins = lax.axis_size("tp")
    here = lax.axis_index("sp")
    half = count // 2
    capacity = 2 * length // count
    planes = [[g * heads + j for j in range(heads)] for g in range(count // heads)]
    halves = [[h * half + j for j in range(half)] for h in range(2)]
    mirror = [(i, i ^ (count - count // 4)) for i in range(count)]
    swap = [(i, twins - 1 - i) for i in range(twins)]

    value_dim = value_rows.shape[1] // heads
    id_rows = jnp.broadcast_to((documents + 1).astype(BF)[None, :], (16, length))
    pairs = pack(key_rows, value_rows, id_rows, heads)
    pairs = lax.all_to_all(pairs, "sp", 0, 0, tiled=True, axis_index_groups=planes)
    queries = jnp.moveaxis(query_rows.reshape(length, heads, value_dim), 1, 0)
    queries = lax.all_to_all(queries, "sp", 0, 0, tiled=True, axis_index_groups=planes)
    prev = lax.ppermute(
        pairs[heads - REACH :], "sp", [(i, i + heads) for i in range(count - heads)]
    )
    following = lax.ppermute(pairs[:REACH], "sp", [(i + heads, i) for i in range(count - heads)])

    ranks = ranks_of(routes, count)
    my_half = here // half
    meta_own = meta_of(routes, ranks, route_weights, my_half * half, half, capacity)
    meta_far = meta_of(routes, ranks, route_weights, (1 - my_half) * half, half, capacity)
    meta_far = lax.ppermute(meta_far, "sp", mirror)
    prev, following, residual_late = lax.optimization_barrier((prev, following, residual))
    residual_far = lax.ppermute(residual_late, "sp", mirror)

    own = (gate_weight[0], up_weight[0], down_weight[0])
    other = tuple(lax.ppermute(weight, "tp", swap) for weight in own)

    lam = lax.dynamic_slice(mix_lambda, (here % heads,), (1,))
    outs = attention(lam, queries, prev, pairs, following)
    outs = outs.reshape(heads * twins, length // twins, value_dim)
    both = [[g * heads * twins + j for j in range(heads * twins)] for g in range(count // heads)]
    token_heads = lax.all_to_all(
        outs, ("sp", "tp"), 0, 0, tiled=True, axis_index_groups=both
    )
    heads_far = lax.ppermute(token_heads, "sp", mirror)

    gain = norm_gain.reshape(1, width)
    slots = half * capacity

    def exchange(rows):
        rows = rows.reshape(half, capacity, width)
        rows = lax.all_to_all(rows, "sp", 0, 0, tiled=True, axis_index_groups=halves)
        return rows.reshape(slots, width)

    rows_own, mixed = project(token_heads, residual, gain, meta_own, out_weight, slots, True)
    rows_own = exchange(rows_own)
    rows_far = project(heads_far, residual_far, gain, meta_far, out_weight, slots, False)
    rows_far = exchange(rows_far)
    answer_own = experts_of(rows_own, own, other)
    answer_far = experts_of(rows_far, own, other)
    back_far = exchange(answer_far)
    part_far = partial_sum(meta_far, back_far)
    part = lax.ppermute(part_far, "sp", mirror)
    back_own = exchange(answer_own)
    return final_sum(meta_own, back_own, mixed, part)


def solution(mesh):
    placed = (
        P(("sp", "tp"), None),
        P("sp", "tp"),
        P("sp", "tp"),
        P("sp", "tp"),
        P("tp"),
        P("sp"),
        P(),
        P(),
        P("sp", None, "tp"),
        P("sp", None, "tp"),
        P("sp", "tp", None),
        P(("sp", "tp"), None),
        P(("sp", "tp"), None),
    )
    return jax.shard_map(
        on_device, mesh=mesh, in_specs=placed, out_specs=P(("sp", "tp"), None), check_vma=False
    )
```

```python
import functools

import jax
import jax.numpy as jnp
from jax import lax
from jax.experimental import pallas as pl
from jax.experimental.pallas import tpu as pltpu
from jax.sharding import PartitionSpec as P


HD = 64
REACH = 3
EPS = 1e-06
BF = jnp.bfloat16
F32 = jnp.float32
VM = pl.BlockSpec(memory_space=pltpu.VMEM)
SM = pl.BlockSpec(memory_space=pltpu.SMEM)
ANY = pl.BlockSpec(memory_space=pl.ANY)


def params(mebibytes):
    return pltpu.CompilerParams(vmem_limit_bytes=mebibytes * 1024 * 1024)


def in_hbm(value):
    return pltpu.with_memory_space_constraint(value, pltpu.HBM)


def cost(flops, bytes_accessed):
    return pl.CostEstimate(flops=flops, bytes_accessed=bytes_accessed, transcendentals=0)


def pack_kernel(k_ref, v_ref, id_ref, o_ref):
    heads, rows, width = o_ref.shape
    length = k_ref.shape[0]
    part = width // 2
    ids = jnp.broadcast_to((id_ref[...] + 1).astype(F32)[None, :], (rows - length, width)).astype(BF)
    for h in range(heads):
        columns = slice(h * part, (h + 1) * part)
        o_ref[h, :length, :part] = k_ref[:, columns]
        o_ref[h, :length, part:] = v_ref[:, columns]
        o_ref[h, length:, :] = ids


def pack(key_rows, value_rows, documents, heads):
    length = key_rows.shape[0]
    width = key_rows.shape[1] // heads
    return pl.pallas_call(
        pack_kernel,
        in_specs=[VM] * 3,
        out_specs=VM,
        out_shape=jax.ShapeDtypeStruct((heads, length + 16, 2 * width), BF),
        compiler_params=params(8),
        name="pack",
    )(in_hbm(key_rows), in_hbm(value_rows), in_hbm(documents))


def attention_kernel(
    lam_ref,
    q_ref,
    prev_ref,
    own_ref,
    next_ref,
    o_ref,
    k_ref,
    v_ref,
    line_ref,
    id_ref,
    bound_ref,
):
    b = pl.program_id(0)
    length, width = o_ref.shape[1:]
    before, group, after = prev_ref.shape[0], own_ref.shape[0], next_ref.shape[0]
    span = before + 1 + after
    blocks = before + group + after

    @pl.when(b == 0)
    def _():
        id_ref[...] = jnp.zeros_like(id_ref)
        for first, ref in ((0, prev_ref), (before, own_ref), (before + group, next_ref)):
            for i in range(ref.shape[0]):
                rows = slice((first + i) * length, (first + i + 1) * length)
                k_ref[rows, :] = ref[i, :length, :width]
                v_ref[rows, :width] = ref[i, :length, width:]
                named = ref[i, length : length + 16, :].astype(F32)[:1]
                id_ref[first + i : first + i + 1, :] = named
                line_ref[0:1, rows] = named
        v_ref[:, width:] = jnp.ones((v_ref.shape[0], width), BF)
        k_ref[blocks * length :, :] = jnp.zeros((length, width), BF)
        v_ref[blocks * length :, :width] = jnp.zeros((length, width), BF)
        line_ref[0:1, blocks * length :] = jnp.zeros((1, length), F32)

        ids = id_ref[...]
        smallest = jnp.min(ids, axis=1, keepdims=True)
        largest = jnp.max(ids, axis=1, keepdims=True)
        place = lax.broadcasted_iota(jnp.int32, smallest.shape, 0)
        for i in range(group):
            low = smallest[before + i : before + i + 1]
            high = largest[before + i : before + i + 1]
            apart = (largest < low) | (smallest > high)
            early = apart & (place >= i) & (place < i + before)
            late = apart & (place > i + before) & (place < i + span)
            bound_ref[0, i] = jnp.sum(jnp.where(early, 1.0, 0.0)).astype(jnp.int32)
            bound_ref[1, i] = jnp.sum(jnp.where(late, 1.0, 0.0)).astype(jnp.int32)

    query_ids = id_ref[pl.ds(b + before, 1), :]
    left = bound_ref[0, b]
    pairs = (span + 1 - bound_ref[1, b] - left) // 2
    start = pl.multiple_of((b + left) * length, length)
    query_column = jnp.transpose(jnp.broadcast_to(query_ids, (128, length)))
    lam = lam_ref[0]

    def attend(keys):
        named = line_ref[0:1, pl.ds(start, keys)]
        for chunk in range(length // 128):
            mine = query_column[chunk * 128 : (chunk + 1) * 128, :]
            q = q_ref[b, chunk * 128 : (chunk + 1) * 128, :]
            q = (q.astype(F32) * (HD**-0.5)).astype(BF)
            zero = jnp.zeros((128, HD), BF)
            sides = (
                jnp.concatenate([q[:, :HD], zero], axis=1),
                jnp.concatenate([zero, q[:, HD:]], axis=1),
            )
            maps = []
            for side in sides:
                scores = lax.dot_general(
                    side,
                    k_ref[pl.ds(start, keys), :],
                    (((1,), (1,)), ((), ())),
                    preferred_element_type=F32,
                )
                pieces = []
                best = None
                for part in range(keys // 128):
                    columns = slice(part * 128, (part + 1) * 128)
                    piece = jnp.where(mine == named[:, columns], scores[:, columns], -1e30)
                    best = piece if best is None else jnp.maximum(best, piece)
                    pieces.append(piece)
                top = jnp.max(best, axis=1, keepdims=True)
                lifted = jnp.concatenate(
                    [jnp.exp(piece - top).astype(BF) for piece in pieces], axis=1
                )
                total = jnp.dot(
                    lifted, v_ref[pl.ds(start, keys), :], preferred_element_type=F32
                )
                maps.append(total[:, :width] / total[:, width:])
            out = maps[0] - lam * maps[1]
            scale = lax.rsqrt(jnp.mean(out * out, axis=1, keepdims=True) + EPS)
            o_ref[b, chunk * 128 : (chunk + 1) * 128, :] = (out * scale).astype(BF)

    for count in range(1, (span + 1) // 2 + 1):

        @pl.when(pairs == count)
        def _():
            attend(count * 2 * length)


def attention(lam, queries, prev, own, following):
    group, length, width = queries.shape
    before, after = prev.shape[0], following.shape[0]
    blocks = before + group + after
    return pl.pallas_call(
        attention_kernel,
        grid=(group,),
        in_specs=[SM] + [VM] * 4,
        out_specs=VM,
        out_shape=jax.ShapeDtypeStruct((group, length, width), BF),
        scratch_shapes=[
            pltpu.VMEM(((blocks + 1) * length, width), BF),
            pltpu.VMEM(((blocks + 1) * length, 2 * width), BF),
            pltpu.VMEM((8, (blocks + 1) * length), F32),
            pltpu.VMEM((-(-(blocks + 1) // 8) * 8, length), F32),
            pltpu.SMEM((2, group), jnp.int32),
        ],
        compiler_params=params(16),
        cost_estimate=cost(8 * 10**9, 4 * 10**6),
        name="attention",
    )(lam, queries, prev, own, following)


def project_kernel(
    heads_ref,
    residual_ref,
    gain_ref,
    meta_ref,
    weight_ref,
    rows_ref,
    mixed_ref,
    left_ref,
    held_ref,
    sems,
    *,
    tile,
):
    tokens, width = mixed_ref.shape
    arrivals = []
    for n in range(width // tile):
        at = pl.ds(n * tile, tile)
        arrivals.append(
            pltpu.make_async_copy(weight_ref.at[:, at], held_ref.at[:, at], sems.at[n])
        )
        arrivals[n].start()
    members = heads_ref.shape[0]
    value_dim = heads_ref.shape[2]
    for source in range(members):
        head = (source % 2) * (members // 2) + source // 2
        left_ref[:, head * value_dim : (head + 1) * value_dim] = heads_ref[source]
    squares = jnp.zeros((tokens, 128), F32)
    for n in range(width // tile):
        columns = slice(n * tile, (n + 1) * tile)
        arrivals[n].wait()
        projected = jnp.dot(left_ref[...], held_ref[:, columns], preferred_element_type=F32)
        mixed = (residual_ref[:, columns].astype(F32) + projected).astype(BF)
        mixed_ref[:, columns] = mixed
        wide = mixed.astype(F32)
        wide = wide * wide
        for part in range(tile // 128):
            squares = squares + wide[:, part * 128 : (part + 1) * 128]
    scale = lax.rsqrt(jnp.sum(squares, axis=1, keepdims=True) / width + EPS)
    slots = rows_ref.shape[0]
    place = lax.broadcasted_iota(jnp.int32, (slots, tokens), 0).astype(F32)
    pick = (place == meta_ref[0:1, :]) | (place == meta_ref[1:2, :])
    pick = jnp.where(pick, 1.0, 0.0).astype(BF)
    for n in range(width // tile):
        columns = slice(n * tile, (n + 1) * tile)
        normed = mixed_ref[:, columns].astype(F32) * scale * gain_ref[:, columns]
        rows_ref[:, columns] = jnp.dot(
            pick, normed.astype(BF), preferred_element_type=F32
        ).astype(BF)


def project(heads, residual, gain, meta, out_weight, slots, keep, tile=512):
    _, tokens, _ = heads.shape
    depth, width = out_weight.shape
    rows = jax.ShapeDtypeStruct((slots, width), BF)
    mixed = pltpu.HBM((tokens, width), BF)
    scratch = [
        pltpu.VMEM((tokens, depth), BF),
        pltpu.VMEM((depth, width), BF),
        pltpu.SemaphoreType.DMA((width // tile,)),
    ]
    return pl.pallas_call(
        functools.partial(project_kernel, tile=tile),
        in_specs=[VM] * 4 + [ANY],
        out_specs=[VM, VM] if keep else VM,
        out_shape=[rows, mixed] if keep else rows,
        scratch_shapes=scratch if keep else [pltpu.VMEM((tokens, width), BF), *scratch],
        compiler_params=params(16),
        cost_estimate=cost(3 * 10**9, 8 * 10**6),
    )(heads, residual, gain, meta, in_hbm(out_weight))


def expert_rows(x_ref, g, u, d, y_ref, hidden_ref, half_ref, tile, arrive):
    halves, width, depth = g.shape
    for h in range(halves):
        for step in range(depth // tile):
            at = slice(step * tile, (step + 1) * tile)
            arrive(h, step)
            gate = jnp.dot(x_ref[...], g[h, :, at], preferred_element_type=F32)
            upward = jnp.dot(x_ref[...], u[h, :, at], preferred_element_type=F32)
            hidden_ref[:, at] = (gate / (1.0 + jnp.exp(-gate)) * upward).astype(BF)
        arrive(h, depth // tile)
        for n in range(width // tile):
            at = slice(n * tile, (n + 1) * tile)
            part = jnp.dot(hidden_ref[...], d[h, :, at], preferred_element_type=F32).astype(BF)
            if h:
                y_ref[:, at] = (half_ref[:, at].astype(F32) + part.astype(F32)).astype(BF)
            else:
                half_ref[:, at] = part


def expert_kernel(
    x_ref, g0, u0, d0, g1, u1, d1, y_ref, gs, us, ds, hidden_ref, half_ref, sems, *, tile
):
    steps = g0.shape[1] // tile
    arrivals = []
    for h, (g, u, d) in enumerate(((g0, u0, d0), (g1, u1, d1))):
        waves = []
        for step in range(steps):
            at = pl.ds(step * tile, tile)
            waves.append(
                (
                    pltpu.make_async_copy(g.at[:, at], gs.at[h, :, at], sems.at[h, 2 * step]),
                    pltpu.make_async_copy(u.at[:, at], us.at[h, :, at], sems.at[h, 2 * step + 1]),
                )
            )
        waves.append((pltpu.make_async_copy(d, ds.at[h], sems.at[h, 2 * steps]),))
        arrivals.append(waves)
    for waves in arrivals:
        for wave in waves:
            for copy in wave:
                copy.start()

    def arrive(h, step):
        for copy in arrivals[h][step]:
            copy.wait()

    expert_rows(x_ref, gs, us, ds, y_ref, hidden_ref, half_ref, tile, arrive)


def experts_of(x, own, other, tile=256):
    rows, width = x.shape
    depth = own[0].shape[1]
    return pl.pallas_call(
        functools.partial(expert_kernel, tile=tile),
        in_specs=[VM] + [ANY] * 6,
        out_specs=VM,
        out_shape=jax.ShapeDtypeStruct((rows, width), BF),
        scratch_shapes=[
            pltpu.VMEM((2, width, depth), BF),
            pltpu.VMEM((2, width, depth), BF),
            pltpu.VMEM((2, depth, width), BF),
            pltpu.VMEM((rows, depth), BF),
            pltpu.VMEM((rows, width), BF),
            pltpu.SemaphoreType.DMA((2, 2 * (depth // tile) + 1)),
        ],
        compiler_params=params(40),
        cost_estimate=cost(9 * 10**9, 26 * 10**6),
    )(x, *(in_hbm(weight) for weight in (*own, *other)))


def picked(meta_ref, rows_ref, write, tile=512):
    slots, width = rows_ref.shape
    tokens = meta_ref.shape[1]
    columns = jnp.transpose(meta_ref[...])
    place = lax.broadcasted_iota(jnp.int32, (tokens, slots), 1).astype(F32)
    picks = jnp.concatenate(
        [jnp.where(place == columns[:, k : k + 1], 1.0, 0.0) for k in range(2)], axis=0
    ).astype(BF)
    for n in range(width // tile):
        at = slice(n * tile, (n + 1) * tile)
        rows = jnp.dot(picks, rows_ref[:, at], preferred_element_type=F32)
        write(at, rows[:tokens] * columns[:, 2:3] + rows[tokens:] * columns[:, 3:4])


def partial_kernel(meta_ref, rows_ref, o_ref):
    def write(at, total):
        o_ref[:, at] = total.astype(BF)

    picked(meta_ref, rows_ref, write)


def final_kernel(meta_ref, rows_ref, mixed_ref, far_ref, o_ref):
    def write(at, total):
        total = total + far_ref[:, at].astype(F32)
        o_ref[:, at] = (mixed_ref[:, at].astype(F32) + total).astype(BF)

    picked(meta_ref, rows_ref, write)


def partial_sum(meta, rows):
    return pl.pallas_call(
        partial_kernel,
        in_specs=[VM] * 2,
        out_specs=VM,
        out_shape=jax.ShapeDtypeStruct((meta.shape[1], rows.shape[1]), BF),
        compiler_params=params(12),
        cost_estimate=cost(10**9, 2 * 10**6),
        name="partial_sum",
    )(meta, rows)


def final_sum(meta, rows, mixed, far):
    return pl.pallas_call(
        final_kernel,
        in_specs=[VM] * 4,
        out_specs=VM,
        out_shape=jax.ShapeDtypeStruct(mixed.shape, BF),
        compiler_params=params(12),
        cost_estimate=cost(10**9, 3 * 10**6),
        name="final_sum",
    )(meta, rows, mixed, far)


def ranks_of(routes, experts):
    tokens = routes.shape[0]
    table = (routes[:, :, None] == jnp.arange(experts, dtype=jnp.int32)).astype(F32)
    named = jnp.sum(table, axis=1)
    order = jnp.arange(tokens)
    below = (order[:, None] > order[None, :]).astype(BF)
    earlier = jnp.dot(below, named.astype(BF), preferred_element_type=F32)
    return jnp.sum(earlier[:, None, :] * table, axis=2)


def meta_of(routes, ranks, route_weights, first, count, capacity):
    local = routes - first
    inside = (local >= 0) & (local < count)
    target = jnp.where(inside, local.astype(F32) * capacity + ranks, -1.0)
    rows = jnp.concatenate([target.T, route_weights.T], axis=0)
    return jnp.concatenate([rows, jnp.zeros((8 - rows.shape[0], rows.shape[1]), F32)], axis=0)


def on_device(
    residual,
    query_rows,
    key_rows,
    value_rows,
    mix_lambda,
    documents,
    out_weight,
    norm_gain,
    gate_weight,
    up_weight,
    down_weight,
    routes,
    route_weights,
):
    length = query_rows.shape[0]
    heads = mix_lambda.shape[0]
    width = residual.shape[1]
    count = lax.axis_size("sp")
    twins = lax.axis_size("tp")
    here = lax.axis_index("sp")
    half = count // 2
    capacity = 2 * length // count
    planes = [[g * heads + j for j in range(heads)] for g in range(count // heads)]
    halves = [[h * half + j for j in range(half)] for h in range(2)]
    mirror = [(i, i ^ (count - count // 4)) for i in range(count)]
    swap = [(i, twins - 1 - i) for i in range(twins)]

    value_dim = value_rows.shape[1] // heads
    pairs = pack(key_rows, value_rows, documents, heads)
    pairs = lax.all_to_all(pairs, "sp", 0, 0, tiled=True, axis_index_groups=planes)
    queries = jnp.moveaxis(query_rows.reshape(length, heads, value_dim), 1, 0)
    queries = lax.all_to_all(queries, "sp", 0, 0, tiled=True, axis_index_groups=planes)
    prev = lax.ppermute(
        pairs[heads - REACH :], "sp", [(i, i + heads) for i in range(count - heads)]
    )
    following = lax.ppermute(pairs[:REACH], "sp", [(i + heads, i) for i in range(count - heads)])

    ranks = ranks_of(routes, count)
    my_half = here // half
    meta_own = meta_of(routes, ranks, route_weights, my_half * half, half, capacity)
    meta_far = meta_of(routes, ranks, route_weights, (1 - my_half) * half, half, capacity)
    meta_far = lax.ppermute(meta_far, "sp", mirror)
    prev, residual_late = lax.optimization_barrier((prev, residual))
    residual_far = lax.ppermute(residual_late, "sp", mirror)

    own = (gate_weight[0], up_weight[0], down_weight[0])
    other = tuple(lax.ppermute(weight, "tp", swap) for weight in own)

    lam = lax.dynamic_slice(mix_lambda, (here % heads,), (1,))
    outs = attention(lam, queries, prev, pairs, following)
    outs = outs.reshape(heads * twins, length // twins, value_dim)
    both = [[g * heads * twins + j for j in range(heads * twins)] for g in range(count // heads)]
    token_heads = lax.all_to_all(
        outs, ("sp", "tp"), 0, 0, tiled=True, axis_index_groups=both
    )
    heads_far = lax.ppermute(token_heads, "sp", mirror)

    gain = norm_gain.reshape(1, width)
    slots = half * capacity

    def exchange(rows):
        rows = rows.reshape(half, capacity, width)
        rows = lax.all_to_all(rows, "sp", 0, 0, tiled=True, axis_index_groups=halves)
        return rows.reshape(slots, width)

    rows_own, mixed = project(token_heads, residual, gain, meta_own, out_weight, slots, True)
    rows_own = exchange(rows_own)
    rows_far = project(heads_far, residual_far, gain, meta_far, out_weight, slots, False)
    rows_far = exchange(rows_far)
    answer_own = experts_of(rows_own, own, other)
    answer_far = experts_of(rows_far, own, other)
    back_far = exchange(answer_far)
    part_far = partial_sum(meta_far, back_far)
    part = lax.ppermute(part_far, "sp", mirror)
    back_own = exchange(answer_own)
    return final_sum(meta_own, back_own, mixed, part)


def solution(mesh):
    placed = (
        P(("sp", "tp"), None),
        P("sp", "tp"),
        P("sp", "tp"),
        P("sp", "tp"),
        P("tp"),
        P("sp"),
        P(),
        P(),
        P("sp", None, "tp"),
        P("sp", None, "tp"),
        P("sp", "tp", None),
        P(("sp", "tp"), None),
        P(("sp", "tp"), None),
    )
    return jax.shard_map(
        on_device, mesh=mesh, in_specs=placed, out_specs=P(("sp", "tp"), None), check_vma=False
    )
```

```python
import functools

import jax
import jax.numpy as jnp
from jax import lax
from jax.experimental import pallas as pl
from jax.experimental.pallas import tpu as pltpu
from jax.sharding import PartitionSpec as P


HD = 64
REACH = 3
EPS = 1e-06
BF = jnp.bfloat16
F32 = jnp.float32
VM = pl.BlockSpec(memory_space=pltpu.VMEM)
SM = pl.BlockSpec(memory_space=pltpu.SMEM)
ANY = pl.BlockSpec(memory_space=pl.ANY)


def params(mebibytes):
    return pltpu.CompilerParams(vmem_limit_bytes=mebibytes * 1024 * 1024)


def in_hbm(value):
    return pltpu.with_memory_space_constraint(value, pltpu.HBM)


def cost(flops, bytes_accessed):
    return pl.CostEstimate(flops=flops, bytes_accessed=bytes_accessed, transcendentals=0)


def pack_kernel(k_ref, v_ref, id_ref, o_ref):
    heads, rows, width = o_ref.shape
    length = k_ref.shape[0]
    part = width // 2
    ids = jnp.broadcast_to((id_ref[...] + 1).astype(F32)[None, :], (rows - length, width)).astype(BF)
    for h in range(heads):
        columns = slice(h * part, (h + 1) * part)
        o_ref[h, :length, :part] = k_ref[:, columns]
        o_ref[h, :length, part:] = v_ref[:, columns]
        o_ref[h, length:, :] = ids


def pack(key_rows, value_rows, documents, heads):
    length = key_rows.shape[0]
    width = key_rows.shape[1] // heads
    return pl.pallas_call(
        pack_kernel,
        in_specs=[VM] * 3,
        out_specs=VM,
        out_shape=jax.ShapeDtypeStruct((heads, length + 16, 2 * width), BF),
        compiler_params=params(8),
        name="pack",
    )(in_hbm(key_rows), in_hbm(value_rows), in_hbm(documents))


def attention_kernel(
    lam_ref,
    q_ref,
    prev_ref,
    own_ref,
    next_ref,
    o_ref,
    k_ref,
    v_ref,
    line_ref,
    id_ref,
    bound_ref,
):
    b = pl.program_id(0)
    length, width = o_ref.shape[1:]
    before, group, after = prev_ref.shape[0], own_ref.shape[0], next_ref.shape[0]
    span = before + 1 + after

    @pl.when(b == 0)
    def _():
        id_ref[...] = jnp.zeros_like(id_ref)
        for first, ref in ((0, prev_ref), (before, own_ref), (before + group, next_ref)):
            for i in range(ref.shape[0]):
                rows = slice((first + i) * length, (first + i + 1) * length)
                k_ref[rows, :] = ref[i, :length, :width]
                v_ref[rows, :width] = ref[i, :length, width:]
                named = ref[i, length : length + 16, :].astype(F32)[:1]
                id_ref[first + i : first + i + 1, :] = named
                line_ref[0:1, rows] = named
        v_ref[:, width:] = jnp.ones((v_ref.shape[0], width), BF)

        ids = id_ref[...]
        smallest = jnp.min(ids, axis=1, keepdims=True)
        largest = jnp.max(ids, axis=1, keepdims=True)
        place = lax.broadcasted_iota(jnp.int32, smallest.shape, 0)
        for i in range(group):
            low = smallest[before + i : before + i + 1]
            high = largest[before + i : before + i + 1]
            apart = (largest < low) | (smallest > high)
            early = apart & (place >= i) & (place < i + before)
            late = apart & (place > i + before) & (place < i + span)
            bound_ref[0, i] = jnp.sum(jnp.where(early, 1.0, 0.0)).astype(jnp.int32)
            bound_ref[1, i] = jnp.sum(jnp.where(late, 1.0, 0.0)).astype(jnp.int32)

    query_ids = id_ref[pl.ds(b + before, 1), :]
    left = bound_ref[0, b]
    needed = span - bound_ref[1, b] - left
    start = pl.multiple_of((b + left) * length, length)
    query_column = jnp.transpose(jnp.broadcast_to(query_ids, (128, length)))
    lam = lam_ref[0]

    def attend(keys):
        named = line_ref[0:1, pl.ds(start, keys)]
        for chunk in range(length // 128):
            mine = query_column[chunk * 128 : (chunk + 1) * 128, :]
            q = q_ref[b, chunk * 128 : (chunk + 1) * 128, :]
            q = (q.astype(F32) * (HD**-0.5)).astype(BF)
            zero = jnp.zeros((128, HD), BF)
            sides = (
                jnp.concatenate([q[:, :HD], zero], axis=1),
                jnp.concatenate([zero, q[:, HD:]], axis=1),
            )
            maps = []
            for side in sides:
                scores = lax.dot_general(
                    side,
                    k_ref[pl.ds(start, keys), :],
                    (((1,), (1,)), ((), ())),
                    preferred_element_type=F32,
                )
                pieces = []
                best = None
                for part in range(keys // 128):
                    columns = slice(part * 128, (part + 1) * 128)
                    piece = jnp.where(mine == named[:, columns], scores[:, columns], -1e30)
                    best = piece if best is None else jnp.maximum(best, piece)
                    pieces.append(piece)
                top = jnp.max(best, axis=1, keepdims=True)
                lifted = jnp.concatenate(
                    [jnp.exp(piece - top).astype(BF) for piece in pieces], axis=1
                )
                total = jnp.dot(
                    lifted, v_ref[pl.ds(start, keys), :], preferred_element_type=F32
                )
                maps.append(total[:, :width] / total[:, width:])
            out = maps[0] - lam * maps[1]
            scale = lax.rsqrt(jnp.mean(out * out, axis=1, keepdims=True) + EPS)
            o_ref[b, chunk * 128 : (chunk + 1) * 128, :] = (out * scale).astype(BF)

    for count in range(1, span + 1):

        @pl.when(needed == count)
        def _():
            attend(count * length)


def attention(lam, queries, prev, own, following):
    group, length, width = queries.shape
    before, after = prev.shape[0], following.shape[0]
    blocks = before + group + after
    return pl.pallas_call(
        attention_kernel,
        grid=(group,),
        in_specs=[SM] + [VM] * 4,
        out_specs=VM,
        out_shape=jax.ShapeDtypeStruct((group, length, width), BF),
        scratch_shapes=[
            pltpu.VMEM((blocks * length, width), BF),
            pltpu.VMEM((blocks * length, 2 * width), BF),
            pltpu.VMEM((8, blocks * length), F32),
            pltpu.VMEM((-(-blocks // 8) * 8, length), F32),
            pltpu.SMEM((2, group), jnp.int32),
        ],
        compiler_params=params(16),
        cost_estimate=cost(8 * 10**9, 4 * 10**6),
        name="attention",
    )(lam, queries, prev, own, following)


def project_kernel(
    heads_ref,
    residual_ref,
    gain_ref,
    meta_ref,
    weight_ref,
    rows_ref,
    mixed_ref,
    left_ref,
    held_ref,
    sems,
    *,
    tile,
):
    tokens, width = mixed_ref.shape
    arrivals = []
    for n in range(width // tile):
        at = pl.ds(n * tile, tile)
        arrivals.append(
            pltpu.make_async_copy(weight_ref.at[:, at], held_ref.at[:, at], sems.at[n])
        )
        arrivals[n].start()
    members = heads_ref.shape[0]
    value_dim = heads_ref.shape[2]
    for source in range(members):
        head = (source % 2) * (members // 2) + source // 2
        left_ref[:, head * value_dim : (head + 1) * value_dim] = heads_ref[source]
    squares = jnp.zeros((tokens, 128), F32)
    for n in range(width // tile):
        columns = slice(n * tile, (n + 1) * tile)
        arrivals[n].wait()
        projected = jnp.dot(left_ref[...], held_ref[:, columns], preferred_element_type=F32)
        mixed = (residual_ref[:, columns].astype(F32) + projected).astype(BF)
        mixed_ref[:, columns] = mixed
        wide = mixed.astype(F32)
        wide = wide * wide
        for part in range(tile // 128):
            squares = squares + wide[:, part * 128 : (part + 1) * 128]
    scale = lax.rsqrt(jnp.sum(squares, axis=1, keepdims=True) / width + EPS)
    slots = rows_ref.shape[0]
    place = lax.broadcasted_iota(jnp.int32, (slots, tokens), 0).astype(F32)
    pick = (place == meta_ref[0:1, :]) | (place == meta_ref[1:2, :])
    pick = jnp.where(pick, 1.0, 0.0).astype(BF)
    for n in range(width // tile):
        columns = slice(n * tile, (n + 1) * tile)
        normed = mixed_ref[:, columns].astype(F32) * scale * gain_ref[:, columns]
        rows_ref[:, columns] = jnp.dot(
            pick, normed.astype(BF), preferred_element_type=F32
        ).astype(BF)


def project(heads, residual, gain, meta, out_weight, slots, keep, tile=512):
    _, tokens, _ = heads.shape
    depth, width = out_weight.shape
    rows = jax.ShapeDtypeStruct((slots, width), BF)
    mixed = pltpu.HBM((tokens, width), BF)
    scratch = [
        pltpu.VMEM((tokens, depth), BF),
        pltpu.VMEM((depth, width), BF),
        pltpu.SemaphoreType.DMA((width // tile,)),
    ]
    return pl.pallas_call(
        functools.partial(project_kernel, tile=tile),
        in_specs=[VM] * 4 + [ANY],
        out_specs=[VM, VM] if keep else VM,
        out_shape=[rows, mixed] if keep else rows,
        scratch_shapes=scratch if keep else [pltpu.VMEM((tokens, width), BF), *scratch],
        compiler_params=params(16),
        cost_estimate=cost(3 * 10**9, 8 * 10**6),
    )(heads, residual, gain, meta, in_hbm(out_weight))


def expert_rows(x_ref, g, u, d, y_ref, hidden_ref, half_ref, tile, wide, arrive):
    halves, width, depth = g.shape
    for h in range(halves):
        for step in range(depth // tile):
            at = slice(step * tile, (step + 1) * tile)
            arrive(h, step)
            gate = jnp.dot(x_ref[...], g[h, :, at], preferred_element_type=F32)
            upward = jnp.dot(x_ref[...], u[h, :, at], preferred_element_type=F32)
            hidden_ref[:, at] = (gate / (1.0 + jnp.exp(-gate)) * upward).astype(BF)
        arrive(h, depth // tile)
        for n in range(width // wide):
            at = slice(n * wide, (n + 1) * wide)
            part = jnp.dot(hidden_ref[...], d[h, :, at], preferred_element_type=F32).astype(BF)
            if h:
                y_ref[:, at] = (half_ref[:, at].astype(F32) + part.astype(F32)).astype(BF)
            else:
                half_ref[:, at] = part


def expert_kernel(
    x_ref, g0, u0, d0, g1, u1, d1, y_ref, gs, us, ds, hidden_ref, half_ref, sems, *, tile, wide
):
    steps = g0.shape[1] // tile
    arrivals = []
    for h, (g, u, d) in enumerate(((g0, u0, d0), (g1, u1, d1))):
        waves = []
        for step in range(steps):
            at = pl.ds(step * tile, tile)
            waves.append(
                (
                    pltpu.make_async_copy(g.at[:, at], gs.at[h, :, at], sems.at[h, 2 * step]),
                    pltpu.make_async_copy(u.at[:, at], us.at[h, :, at], sems.at[h, 2 * step + 1]),
                )
            )
        waves.append((pltpu.make_async_copy(d, ds.at[h], sems.at[h, 2 * steps]),))
        arrivals.append(waves)
    for waves in arrivals:
        for wave in waves:
            for copy in wave:
                copy.start()

    def arrive(h, step):
        for copy in arrivals[h][step]:
            copy.wait()

    expert_rows(x_ref, gs, us, ds, y_ref, hidden_ref, half_ref, tile, wide, arrive)


def experts_of(x, own, other, tile=512, wide=1024):
    rows, width = x.shape
    depth = own[0].shape[1]
    return pl.pallas_call(
        functools.partial(expert_kernel, tile=tile, wide=wide),
        in_specs=[VM] + [ANY] * 6,
        out_specs=VM,
        out_shape=jax.ShapeDtypeStruct((rows, width), BF),
        scratch_shapes=[
            pltpu.VMEM((2, width, depth), BF),
            pltpu.VMEM((2, width, depth), BF),
            pltpu.VMEM((2, depth, width), BF),
            pltpu.VMEM((rows, depth), BF),
            pltpu.VMEM((rows, width), BF),
            pltpu.SemaphoreType.DMA((2, 2 * (depth // tile) + 1)),
        ],
        compiler_params=params(40),
        cost_estimate=cost(9 * 10**9, 26 * 10**6),
    )(x, *(in_hbm(weight) for weight in (*own, *other)))


def picked(meta_ref, rows_ref, write, tile=512):
    slots, width = rows_ref.shape
    tokens = meta_ref.shape[1]
    columns = jnp.transpose(meta_ref[...])
    place = lax.broadcasted_iota(jnp.int32, (tokens, slots), 1).astype(F32)
    picks = jnp.concatenate(
        [jnp.where(place == columns[:, k : k + 1], 1.0, 0.0) for k in range(2)], axis=0
    ).astype(BF)
    for n in range(width // tile):
        at = slice(n * tile, (n + 1) * tile)
        rows = jnp.dot(picks, rows_ref[:, at], preferred_element_type=F32)
        write(at, rows[:tokens] * columns[:, 2:3] + rows[tokens:] * columns[:, 3:4])


def partial_kernel(meta_ref, rows_ref, o_ref):
    def write(at, total):
        o_ref[:, at] = total.astype(BF)

    picked(meta_ref, rows_ref, write)


def final_kernel(meta_ref, rows_ref, mixed_ref, far_ref, o_ref):
    def write(at, total):
        total = total + far_ref[:, at].astype(F32)
        o_ref[:, at] = (mixed_ref[:, at].astype(F32) + total).astype(BF)

    picked(meta_ref, rows_ref, write)


def partial_sum(meta, rows):
    return pl.pallas_call(
        partial_kernel,
        in_specs=[VM] * 2,
        out_specs=VM,
        out_shape=jax.ShapeDtypeStruct((meta.shape[1], rows.shape[1]), BF),
        compiler_params=params(12),
        cost_estimate=cost(10**9, 2 * 10**6),
        name="partial_sum",
    )(meta, rows)


def final_sum(meta, rows, mixed, far):
    return pl.pallas_call(
        final_kernel,
        in_specs=[VM] * 4,
        out_specs=VM,
        out_shape=jax.ShapeDtypeStruct(mixed.shape, BF),
        compiler_params=params(12),
        cost_estimate=cost(10**9, 3 * 10**6),
        name="final_sum",
    )(meta, rows, mixed, far)


def ranks_of(routes, experts):
    tokens = routes.shape[0]
    table = (routes[:, :, None] == jnp.arange(experts, dtype=jnp.int32)).astype(F32)
    named = jnp.sum(table, axis=1)
    order = jnp.arange(tokens)
    below = (order[:, None] > order[None, :]).astype(BF)
    earlier = jnp.dot(below, named.astype(BF), preferred_element_type=F32)
    return jnp.sum(earlier[:, None, :] * table, axis=2)


def meta_of(routes, ranks, route_weights, first, count, capacity):
    local = routes - first
    inside = (local >= 0) & (local < count)
    target = jnp.where(inside, local.astype(F32) * capacity + ranks, -1.0)
    rows = jnp.concatenate([target.T, route_weights.T], axis=0)
    return jnp.concatenate([rows, jnp.zeros((8 - rows.shape[0], rows.shape[1]), F32)], axis=0)


def on_device(
    residual,
    query_rows,
    key_rows,
    value_rows,
    mix_lambda,
    documents,
    out_weight,
    norm_gain,
    gate_weight,
    up_weight,
    down_weight,
    routes,
    route_weights,
):
    length = query_rows.shape[0]
    heads = mix_lambda.shape[0]
    width = residual.shape[1]
    count = lax.axis_size("sp")
    twins = lax.axis_size("tp")
    here = lax.axis_index("sp")
    half = count // 2
    capacity = 2 * length // count
    planes = [[g * heads + j for j in range(heads)] for g in range(count // heads)]
    halves = [[h * half + j for j in range(half)] for h in range(2)]
    mirror = [(i, i ^ (count - count // 4)) for i in range(count)]
    swap = [(i, twins - 1 - i) for i in range(twins)]

    value_dim = value_rows.shape[1] // heads
    pairs = pack(key_rows, value_rows, documents, heads)
    pairs = lax.all_to_all(pairs, "sp", 0, 0, tiled=True, axis_index_groups=planes)
    queries = jnp.moveaxis(query_rows.reshape(length, heads, value_dim), 1, 0)
    queries = lax.all_to_all(queries, "sp", 0, 0, tiled=True, axis_index_groups=planes)
    prev = lax.ppermute(
        pairs[heads - REACH :], "sp", [(i, i + heads) for i in range(count - heads)]
    )
    following = lax.ppermute(pairs[:REACH], "sp", [(i + heads, i) for i in range(count - heads)])

    ranks = ranks_of(routes, count)
    my_half = here // half
    meta_own = meta_of(routes, ranks, route_weights, my_half * half, half, capacity)
    meta_far = meta_of(routes, ranks, route_weights, (1 - my_half) * half, half, capacity)
    meta_far = lax.ppermute(meta_far, "sp", mirror)
    prev, residual_late = lax.optimization_barrier((prev, residual))
    residual_far = lax.ppermute(residual_late, "sp", mirror)

    own = (gate_weight[0], up_weight[0], down_weight[0])
    other = tuple(lax.ppermute(weight, "tp", swap) for weight in own)

    lam = lax.dynamic_slice(mix_lambda, (here % heads,), (1,))
    outs = attention(lam, queries, prev, pairs, following)
    outs = outs.reshape(heads * twins, length // twins, value_dim)
    both = [[g * heads * twins + j for j in range(heads * twins)] for g in range(count // heads)]
    token_heads = lax.all_to_all(
        outs, ("sp", "tp"), 0, 0, tiled=True, axis_index_groups=both
    )
    gain = norm_gain.reshape(1, width)
    slots = half * capacity

    def exchange(rows):
        rows = rows.reshape(half, capacity, width)
        rows = lax.all_to_all(rows, "sp", 0, 0, tiled=True, axis_index_groups=halves)
        return rows.reshape(slots, width)

    rows_own, mixed = project(token_heads, residual, gain, meta_own, out_weight, slots, True)
    heads_late, mixed = lax.optimization_barrier((token_heads, mixed))
    heads_far = lax.ppermute(heads_late, "sp", mirror)
    rows_own = exchange(rows_own)
    rows_far = project(heads_far, residual_far, gain, meta_far, out_weight, slots, False)
    rows_far = exchange(rows_far)
    answer_own = experts_of(rows_own, own, other)
    answer_far = experts_of(rows_far, own, other)
    back_far = exchange(answer_far)
    part_far = partial_sum(meta_far, back_far)
    part = lax.ppermute(part_far, "sp", mirror)
    back_own = exchange(answer_own)
    return final_sum(meta_own, back_own, mixed, part)


def solution(mesh):
    placed = (
        P(("sp", "tp"), None),
        P("sp", "tp"),
        P("sp", "tp"),
        P("sp", "tp"),
        P("tp"),
        P("sp"),
        P(),
        P(),
        P("sp", None, "tp"),
        P("sp", None, "tp"),
        P("sp", "tp", None),
        P(("sp", "tp"), None),
        P(("sp", "tp"), None),
    )
    return jax.shard_map(
        on_device, mesh=mesh, in_specs=placed, out_specs=P(("sp", "tp"), None), check_vma=False
    )
```
